256 devices in a mesh: sp: 16 (over y, x), dp: 16 (over z, core).
Axes of the slice: x: 4, y: 4, z: 8, core: 2. Of those that a mesh axis runs over, the one named last changes fastest.
Arguments:
- tokens: bfloat16 [16, 2560, 2048], P('dp', 'sp'), may hold values from -42 to 42
- query_weight: bfloat16 [2048, 1024], P('dp'), may hold values from -1 to 1
- key_weight: bfloat16 [2048, 1024], P('dp'), may hold values from -1 to 1
- values: bfloat16 [16, 2560, 1024], P('dp', 'sp'), may hold values from -6 to 6
- lambdas: float32 [16], replicated, may hold values from 0.3 to 0.8
- out_grad: bfloat16 [16, 2560, 1024], P('dp', 'sp'), may hold values from -6 to 6
Outputs:
- tokens_grad: bfloat16 [16, 2560, 2048], P('dp', 'sp')
- values_grad: bfloat16 [16, 2560, 1024], P('dp', 'sp')
- query_weight_grad: float32 [2048, 1024], P('dp')
- key_weight_grad: float32 [2048, 1024], P('dp')
The draws below stay inside these ranges and needn't reach their ends.
All inputs are finite; a program needn't handle non-finite values.
Results may differ from the reference program's by a relative error of at most 0.029.
The reference program's roundings to bfloat16 on the way count: a program that leaves them out, or rounds other values in their place, can miss the bound.
Values may be sent and summed in bfloat16 or wider, within the bound.
A program may use at most 128 MiB of HBM per device.

```python
import math
import jax
import jax.numpy as jnp
from jax import lax

D = 2048
HEADS = 16
DQK = 32
SEQLEN = 2560
BATCH = 16
QCOLS = 1024
VCOLS = 1024


def weight_normals(key):
    first_draw = jax.random.normal(jax.random.fold_in(key, 11), (D, QCOLS), jnp.float32)
    second_draw = jax.random.normal(jax.random.fold_in(key, 12), (D, QCOLS), jnp.float32)
    return (first_draw, second_draw)


def draw_query_weight(key, part):
    first_draw, second_draw = weight_normals(key)
    return (jnp.clip(first_draw, -6.0, 6.0) * math.sqrt(3.0 / D)).astype(jnp.bfloat16)


def draw_key_weight(key, part):
    first_draw, second_draw = weight_normals(key)
    blended = second_draw
    return (jnp.clip(blended, -6.0, 6.0) * math.sqrt(1.0 / D)).astype(jnp.bfloat16)


def draw_tokens(key, part):
    base_draw = jnp.clip(jax.random.normal(jax.random.fold_in(key, 21), (BATCH, SEQLEN, D), jnp.float32), -6.0, 6.0)
    return base_draw.astype(jnp.bfloat16)


def levels(rng, dims, split, smallest, largest):
    factor_of, own = 1.0, jax.random.fold_in(rng, 6)
    for dim, shards_of in split:
        draws = jnp.exp(jax.random.uniform(jax.random.fold_in(own, dim), (shards_of,), jnp.float32, smallest / len(split), largest / len(split)))
        factor_of = factor_of * jnp.repeat(draws, dims[dim] // shards_of).reshape([-1 if axis == dim else 1 for axis in range(len(dims))])
    return factor_of


def gaussian(own_key, shape, scale, reach, pieces=(), kind=jnp.bfloat16):
    level = levels(own_key, shape, pieces, -0.22, 0.18) if pieces else 1.0
    entries = jax.random.normal(own_key, shape, jnp.float32) * scale * level
    return jnp.minimum(jnp.maximum(entries, -reach), reach).astype(kind)


def setup_inputs(seed: int = 0) -> dict:
    arg_keys = jax.random.split(jax.random.key(seed), 7)
    tokens = draw_tokens(jax.random.fold_in(arg_keys[6], 71), 0)
    query_weight = draw_query_weight(jax.random.fold_in(arg_keys[6], 71), 0)
    key_weight = draw_key_weight(jax.random.fold_in(arg_keys[6], 71), 0)
    values = gaussian(arg_keys[3], (BATCH, SEQLEN, VCOLS), 1.0, 6.0, ((0, 16), (1, 16)))
    lambdas = jnp.clip(jax.random.uniform(arg_keys[4], (HEADS,), jnp.float32, 0.3, 0.8), 0.3, 0.8)
    out_grad = gaussian(arg_keys[5], (BATCH, SEQLEN, VCOLS), 1.0, 6.0, ((0, 16), (1, 16)))
    return dict(tokens=tokens, query_weight=query_weight, key_weight=key_weight, values=values, lambdas=lambdas, out_grad=out_grad)


NORM_EPS = 0.1
THETA = 10000.0

def rotation_tables(positions, vec_width):
    half_width = vec_width // 2
    freqs = jnp.exp(-math.log(THETA) * jnp.arange(half_width, dtype=jnp.float32) / half_width)
    angles = positions.astype(jnp.float32)[:, None] * freqs[None, :]
    return (jnp.cos(angles), jnp.sin(angles))

def rotate(field, cosine, sine_table, vec_width, sign_value):
    full_shape = field.shape
    grouped = field.reshape(full_shape[:-1] + (full_shape[-1] // vec_width, 2, vec_width // 2))
    first_half = grouped[..., 0, :]
    second_half = grouped[..., 1, :]
    cos_cols = cosine[:, None, :]
    sin_cols = sign_value * sine_table[:, None, :]
    turned = jnp.stack([first_half * cos_cols - second_half * sin_cols, second_half * cos_cols + first_half * sin_cols], axis=-2)
    return turned.reshape(full_shape)

def pair_product(pattern, first_op, second_op):
    return jnp.einsum(pattern, first_op.astype(jnp.float32), second_op.astype(jnp.float32))

def head_backward(query_rot, key_rot, value_rows, grad_rows, lambda_here, cosine, sine_table):
    seq_length = query_rot.shape[0]
    head_count = lambda_here.shape[0]
    qk_width = query_rot.shape[1] // (2 * head_count)
    value_width = value_rows.shape[1] // head_count
    block_rows = math.gcd(seq_length, 512)
    block_count = seq_length // block_rows
    inv_root = 1.0 / math.sqrt(qk_width)
    query_split = query_rot.reshape(block_count, block_rows, head_count, 2, qk_width)
    key_split = key_rot.reshape(seq_length, head_count, 2, qk_width)
    value_split = value_rows.reshape(seq_length, head_count, value_width)
    grad_split = grad_rows.reshape(block_count, block_rows, head_count, value_width)
    lambda_col = lambda_here[:, None, None]
    key_positions = jnp.arange(seq_length, dtype=jnp.int32)

    def block_step(carried, inputs):
        key_sum, value_sum = carried
        query_part, grad_part, block_start = inputs
        scores = pair_product('qhmd,khmd->hmqk', query_part, key_split) * inv_root
        query_positions = block_start + jnp.arange(block_rows, dtype=jnp.int32)
        causal_mask = key_positions[None, :] <= query_positions[:, None]
        scores = jnp.where(causal_mask, scores, -jnp.inf)
        row_max = lax.optimization_barrier(jnp.max(scores, axis=-1, keepdims=True))
        exp_scores = jnp.exp(scores - row_max)
        prob_maps = exp_scores / lax.optimization_barrier(jnp.sum(exp_scores, axis=-1, keepdims=True))
        weights = (prob_maps[:, 0] - lambda_col * prob_maps[:, 1]).astype(jnp.bfloat16)
        mixed_out = pair_product('hqk,khe->qhe', weights, value_split)
        norm_scale = lax.rsqrt(lax.optimization_barrier(jnp.mean(mixed_out * mixed_out, axis=-1, keepdims=True)) + NORM_EPS)
        grad_float = grad_part.astype(jnp.float32)
        mixed_grad = (norm_scale * grad_float - norm_scale * norm_scale * norm_scale * mixed_out * lax.optimization_barrier(jnp.mean(grad_float * mixed_out, axis=-1, keepdims=True))).astype(jnp.bfloat16)
        weight_grad = pair_product('qhe,khe->hqk', mixed_grad, value_split)
        value_sum = value_sum + pair_product('hqk,qhe->khe', weights, mixed_grad)
        first_grad = prob_maps[:, 0] * (weight_grad - lax.optimization_barrier(jnp.sum(weight_grad * prob_maps[:, 0], axis=-1, keepdims=True)))
        second_grad = -lambda_col * prob_maps[:, 1] * (weight_grad - lax.optimization_barrier(jnp.sum(weight_grad * prob_maps[:, 1], axis=-1, keepdims=True)))
        score_grad = (jnp.stack([first_grad, second_grad], axis=1) * inv_root).astype(jnp.bfloat16)
        query_grad = pair_product('hmqk,khmd->qhmd', score_grad, key_split)
        key_sum = key_sum + pair_product('hmqk,qhmd->khmd', score_grad, query_part)
        return ((key_sum, value_sum), query_grad)
    zero_init = (jnp.zeros((seq_length, head_count, 2, qk_width), jnp.float32), jnp.zeros((seq_length, head_count, value_width), jnp.float32))
    block_starts = jnp.arange(block_count, dtype=jnp.int32) * block_rows
    (key_sum, value_sum), query_blocks = lax.scan(block_step, zero_init, (query_split, grad_split, block_starts))
    query_turned = query_blocks.reshape(seq_length, head_count * 2 * qk_width)
    key_turned = key_sum.reshape(seq_length, head_count * 2 * qk_width)
    query_back = rotate(query_turned, cosine, sine_table, qk_width, -1.0).astype(jnp.bfloat16)
    key_back = rotate(key_turned, cosine, sine_table, qk_width, -1.0).astype(jnp.bfloat16)
    values_back = value_sum.reshape(seq_length, head_count * value_width).astype(jnp.bfloat16)
    return (query_back, key_back, values_back)

def reference(tokens, query_weight, key_weight, values, lambdas, out_grad):
    cosine, sine_table = rotation_tables(jnp.arange(SEQLEN, dtype=jnp.int32), DQK)
    query_float = query_weight.astype(jnp.float32)
    key_float = key_weight.astype(jnp.float32)

    def one_sequence(inputs):
        token_seq, value_seq, grad_seq = inputs
        token_float = token_seq.astype(jnp.float32)
        query_rot = rotate(jnp.dot(token_float, query_float), cosine, sine_table, DQK, 1.0).astype(jnp.bfloat16)
        key_rot = rotate(jnp.dot(token_float, key_float), cosine, sine_table, DQK, 1.0).astype(jnp.bfloat16)
        query_back, key_back, values_back = head_backward(query_rot, key_rot, value_seq, grad_seq, lambdas, cosine, sine_table)
        query_back_f = query_back.astype(jnp.float32)
        key_back_f = key_back.astype(jnp.float32)
        input_grad = (jnp.dot(query_back_f, query_float.T) + jnp.dot(key_back_f, key_float.T)).astype(jnp.bfloat16)
        query_part = jnp.dot(token_float.T, query_back_f)
        key_part = jnp.dot(token_float.T, key_back_f)
        return (input_grad, values_back, query_part, key_part)
    tokens_grad, values_grad, query_parts, key_parts = lax.map(one_sequence, (tokens, values, out_grad))
    factor = 1.0 / math.sqrt(BATCH * SEQLEN)
    return (tokens_grad, values_grad, lax.optimization_barrier(jnp.sum(query_parts, axis=0)) * factor, lax.optimization_barrier(jnp.sum(key_parts, axis=0)) * factor)
```

```python
import math

import jax
import jax.numpy as jnp
from jax import lax
from jax.experimental import pallas as pl
from jax.experimental.pallas import tpu as pltpu
from jax.sharding import PartitionSpec as P

THETA = 10000.0
DQK = 32
NORM_EPS = 0.1
F32, BF16 = jnp.float32, jnp.bfloat16
SEQ = 2560
BQ = 256
BK = 512
NB = SEQ // BQ


def mm(a, b, dims=(((1,), (0,)), ((), ()))):
    return lax.dot_general(a, b, dims, preferred_element_type=F32)


def rot_t(x, c, s, sign):
    parts = []
    for base in range(0, x.shape[0], 32):
        a, b = x[base:base + 16], x[base + 16:base + 32]
        parts += [a * c - b * (sign * s), b * c + a * (sign * s)]
    return jnp.concatenate(parts, axis=0)


def fold(x, op):
    r = x.reshape(x.shape[0] // 8, 8, x.shape[1])
    return op(r, axis=0)


def attention(lam, rot_ref, rotT_ref, vg_ref, vgT_ref, cosT, sinT, dqT_ref, acc_ref, e1_ref, e2_ref, mix_ref, dp_ref):
    inv_root = 1.0 / math.sqrt(32)
    c2 = inv_root * math.log2(math.e)
    acc_ref[...] = jnp.zeros_like(acc_ref)
    zq = jnp.zeros((32, BQ), BF16)

    def block(step, _):
        b = NB - 1 - step
        qs = pl.multiple_of(b * BQ, BQ)
        qcols = pl.ds(qs, BQ)
        last = b // 2
        q1T = rotT_ref[0:32, qcols]
        q2T = rotT_ref[32:64, qcols]
        rhs1 = jnp.concatenate([zq, zq, q1T, zq], axis=0)
        rhs2 = jnp.concatenate([zq, zq, zq, q2T], axis=0)

        def scores(j):
            ks = pl.multiple_of(j * BK, BK)
            kk = rot_ref[pl.ds(ks, BK), :]
            return ks, mm(kk, rhs1), mm(kk, rhs2)

        def ph1(j, c):
            m1, m2 = c
            ks, s1, s2 = scores(j)
            e1_ref[pl.ds(ks, BK), :] = s1
            e2_ref[pl.ds(ks, BK), :] = s2
            return jnp.maximum(m1, fold(s1, jnp.max)), jnp.maximum(m2, fold(s2, jnp.max))

        neg = jnp.full((8, BQ), -jnp.inf, F32)
        m1, m2 = lax.fori_loop(0, last, ph1, (neg, neg))
        ks, s1, s2 = scores(last)
        mask = (ks + lax.broadcasted_iota(jnp.int32, (BK, BQ), 0)) <= (qs + lax.broadcasted_iota(jnp.int32, (BK, BQ), 1))
        s1 = jnp.where(mask, s1, -jnp.inf)
        s2 = jnp.where(mask, s2, -jnp.inf)
        e1_ref[pl.ds(ks, BK), :] = s1
        e2_ref[pl.ds(ks, BK), :] = s2
        m1 = jnp.max(jnp.maximum(m1, fold(s1, jnp.max)), axis=0, keepdims=True)
        m2 = jnp.max(jnp.maximum(m2, fold(s2, jnp.max)), axis=0, keepdims=True)

        def ph2(j, c):
            l1, l2 = c
            rows = pl.ds(pl.multiple_of(j * BK, BK), BK)
            e1 = jnp.exp2((e1_ref[rows, :] - m1) * c2)
            e2 = jnp.exp2((e2_ref[rows, :] - m2) * c2)
            e1_ref[rows, :] = e1
            e2_ref[rows, :] = e2
            return l1 + fold(e1, jnp.sum), l2 + fold(e2, jnp.sum)

        zero = jnp.zeros((8, BQ), F32)
        l1, l2 = lax.fori_loop(0, last + 1, ph2, (zero, zero))
        r1 = 1.0 / jnp.sum(l1, axis=0, keepdims=True)
        r2 = lam / jnp.sum(l2, axis=0, keepdims=True)

        def ph3(j, o):
            rows = pl.ds(pl.multiple_of(j * BK, BK), BK)
            mix = (e1_ref[rows, :] * r1 - e2_ref[rows, :] * r2).astype(BF16)
            mix_ref[rows, :] = mix
            return o + mm(vgT_ref[0:64, rows], mix)

        o = lax.fori_loop(0, last + 1, ph3, jnp.zeros((64, BQ), F32))
        g = vgT_ref[64:128, qcols].astype(F32)
        ns = lax.rsqrt(jnp.mean(o * o, axis=0, keepdims=True) + NORM_EPS)
        ob = ns * g - ns * ns * ns * o * jnp.mean(g * o, axis=0, keepdims=True)
        obT = ob.astype(BF16)
        obp = jnp.concatenate([jnp.zeros((64, BQ), F32), ob], axis=0).T.astype(BF16)
        obz = jnp.concatenate([obT, jnp.zeros((64, BQ), BF16)], axis=0)

        def ph4(j, c):
            d1, d2 = c
            rows = pl.ds(pl.multiple_of(j * BK, BK), BK)
            dp = mm(vg_ref[rows, :], obz)
            dp_ref[rows, :] = dp
            return d1 + fold(dp * e1_ref[rows, :], jnp.sum), d2 + fold(dp * e2_ref[rows, :], jnp.sum)

        d1, d2 = lax.fori_loop(0, last + 1, ph4, (zero, zero))
        r2n = -r2
        d1 = jnp.sum(d1, axis=0, keepdims=True) * r1
        d2 = jnp.sum(d2, axis=0, keepdims=True) * (1.0 / jnp.sum(l2, axis=0, keepdims=True))
        f1 = r1 * inv_root
        f2 = r2n * inv_root
        lane = lax.broadcasted_iota(jnp.int32, (BQ, 128), 1)
        qrows = rot_ref[qcols, :]
        zb = jnp.zeros_like(qrows)
        rhs = jnp.concatenate([jnp.where(lane < 32, qrows, zb), jnp.where((lane >= 32) & (lane < 64), qrows, zb), obp], axis=0)

        def ph5(j, c):
            a1, a2 = c
            rows = pl.ds(pl.multiple_of(j * BK, BK), BK)
            dp = dp_ref[rows, :]
            g1 = (e1_ref[rows, :] * f1 * (dp - d1)).astype(BF16)
            g2 = (e2_ref[rows, :] * f2 * (dp - d2)).astype(BF16)
            lhs = jnp.concatenate([g1, g2, mix_ref[rows, :]], axis=1)
            acc_ref[rows, :] += mm(lhs, rhs)
            return a1 + mm(rotT_ref[64:96, rows], g1), a2 + mm(rotT_ref[96:128, rows], g2)

        za = jnp.zeros((32, BQ), F32)
        a1, a2 = lax.fori_loop(0, last + 1, ph5, (za, za))
        dqT_ref[0:32, qcols] = a1
        dqT_ref[32:64, qcols] = a2
        return 0

    lax.fori_loop(0, NB, block, 0)


TOK = 160
HALF = 80
D = 2048
COLS = 1024
TRANS_B = (((1,), (1,)), ((), ()))


def spot(q, c):
    q = lax.rem(q + 32, 16)
    u = lax.div(q, 4)
    w = lax.rem(lax.rem(q, 4) - u + 4, 4)
    y = u * (1 - c) + w * c
    x = w * (1 - c) + u * c
    return 4 * y + x


def join(a, b):
    return jnp.concatenate([a[:, :64], b[:, :64]], axis=1), jnp.concatenate([a[:, 64:], b[:, 64:]], axis=1)


def kernel(factor, lam_ref, tok_ref, wq_ref, wk_ref, v_ref, g_ref, cosT, sinT,
           tg_ref, vgrad_ref, dwq_ref, dwk_ref,
           tokF, wqF, wkF, whead, xf, vgpack, vgF, rot, rotT, vgT, dqT, acc, e1, e2, mix, dp,
           backT, bpack, bF, dwp, dwR, dwS, dwG,
           tsend, trecv, wsend, wrecv, psend, precv, asend, arecv, bsend, brecv, rsend, rrecv, gsend, grecv, lsem):
    sp = lax.axis_index("sp")
    dpi = lax.axis_index("dp")
    core = lax.rem(dpi, 2)
    z = lax.div(dpi, 2)
    mate = z * 2 + 1 - core
    y, x = lax.div(sp, 4), lax.rem(sp, 4)
    u = y * (1 - core) + x * core
    w = x * (1 - core) + y * core
    place = 4 * u + lax.rem(u + w, 4)

    barrier = pltpu.get_barrier_semaphore()
    for d in range(1, 16):
        pl.semaphore_signal(barrier, inc=1, device_id={"sp": lax.rem(sp + d, 16)}, device_id_type=pl.DeviceIdType.MESH)
        pl.semaphore_signal(barrier, inc=1, device_id={"dp": lax.rem(dpi + d, 16)}, device_id_type=pl.DeviceIdType.MESH)
    pl.semaphore_wait(barrier, 30)

    sends = []

    def send(src, dst, ss, rs, to):
        c = pltpu.make_async_remote_copy(src_ref=src, dst_ref=dst, send_sem=ss, recv_sem=rs, device_id=to,
                                         device_id_type=pl.DeviceIdType.MESH)
        c.start()
        sends.append(c)

    def arrive(dst, ss, rs):
        pltpu.make_async_remote_copy(src_ref=dst, dst_ref=dst, send_sem=ss, recv_sem=rs, device_id={"sp": sp},
                                     device_id_type=pl.DeviceIdType.MESH).wait_recv()

    nxt = ({"sp": spot(place + 1, core)}, {"sp": spot(place - 1, core)})

    def tok_part(back, d, half):
        origin = spot(place - back, core) if d == 0 else spot(place + back, core)
        return pl.ds(pl.multiple_of(origin * TOK + half * HALF, HALF), HALF)

    def tok_half(d, k):
        return d if k == 14 else k % 2

    def tok_send(d, k):
        half = tok_half(d, k)
        rows = tok_part(k // 2, d, half)
        src = tok_ref.at[pl.ds(half * HALF, HALF)] if k < 2 else tokF.at[rows]
        send(src, tokF.at[rows], tsend.at[d, k], trecv.at[d, k], nxt[d])

    def tok_wait(d, k):
        rows = tok_part(k // 2 + 1, d, tok_half(d, k))
        arrive(tokF.at[rows], tsend.at[d, k], trecv.at[d, k])

    znext = ({"dp": lax.rem(z + 1, 8) * 2 + core}, {"dp": lax.rem(z + 7, 8) * 2 + core})
    wF = (wqF, wkF)
    wown = (wq_ref, wk_ref)

    def w_rows(owner):
        return pl.ds(pl.multiple_of(owner * 128, 128), 128)

    def w_owner(back, d):
        return lax.rem(z + 8 - back, 8) * 2 + core if d == 0 else lax.rem(z + back, 8) * 2 + core

    def w_which(d, k):
        return d if k == 6 else k % 2

    def w_send(d, k):
        m = w_which(d, k)
        rows = w_rows(w_owner(k // 2, d))
        send(wown[m] if k < 2 else wF[m].at[rows], wF[m].at[rows], wsend.at[d, k], wrecv.at[d, k], znext[d])

    def w_wait(d, k):
        arrive(wF[w_which(d, k)].at[w_rows(w_owner(k // 2 + 1, d))], wsend.at[d, k], wrecv.at[d, k])

    def mate_send(d, k):
        if k < 0:
            m, owner, i = d, dpi, 14 + d
        else:
            m, owner, i = w_which(d, k), w_owner(k // 2 + 1, d), d * 7 + k
        rows = w_rows(owner)
        send(wown[m] if k < 0 else wF[m].at[rows], wF[m].at[rows], psend.at[i], precv.at[i], {"dp": mate})

    def mate_wait(d, k):
        if k < 0:
            m, owner, i = d, mate, 14 + d
        else:
            m, owner, i = w_which(d, k), w_owner(k // 2 + 1, d) + 1 - 2 * core, d * 7 + k
        arrive(wF[m].at[w_rows(owner)], psend.at[i], precv.at[i])

    for k in range(2):
        for d in range(2):
            tok_send(d, k)
            w_send(d, k)
    for m in range(2):
        mate_send(m, -1)
    own = [pltpu.make_async_copy(tok_ref, tokF.at[pl.ds(pl.multiple_of(sp * TOK, TOK), TOK)], lsem.at[0]),
           pltpu.make_async_copy(wq_ref, wqF.at[w_rows(dpi)], lsem.at[1]),
           pltpu.make_async_copy(wk_ref, wkF.at[w_rows(dpi)], lsem.at[2])]
    for c in own:
        c.start()

    for p in range(8):
        lanes = slice(p * 128, (p + 1) * 128)
        vp, gp = v_ref[:, lanes], g_ref[:, lanes]
        vgpack[2 * p], vgpack[2 * p + 1] = join(vp, gp)
    vgF[pl.ds(pl.multiple_of(sp * TOK, TOK), TOK), :] = vgpack[sp]
    for c in own:
        c.wait()

    def peer_rows(i, n):
        return pl.ds(pl.multiple_of(i * n, n), n)

    def vg_send():
        for d in range(1, 16):
            to = lax.rem(sp + d, 16)
            send(vgpack.at[to], vgF.at[peer_rows(sp, TOK)], asend.at[d], arecv.at[d], {"sp": to})

    def vg_wait():
        for d in range(1, 16):
            arrive(vgF.at[peer_rows(lax.rem(sp + 16 - d, 16), TOK)], asend.at[d], arecv.at[d])

        def turn(i, _):
            r = pl.multiple_of(i * 256, 256)
            vgT[:, pl.ds(r, 256)] = vgF[pl.ds(r, 256), :].astype(F32).T.astype(BF16)
            return 0
        lax.fori_loop(0, SEQ // 256, turn, 0)

    def make_head():
        pair = pl.ds(pl.multiple_of(lax.div(sp, 2) * 128, 128), 128)
        odd = lax.rem(sp, 2)

        def part(i, _):
            rows = pl.ds(pl.multiple_of(i * 256, 256), 256)
            lo, hi = join(wqF[rows, pair], wkF[rows, pair])
            whead[rows, :] = jnp.where(odd == 0, lo, hi)
            return 0
        lax.fori_loop(0, 8, part, 0)

    def project(origin):
        rows = pl.ds(pl.multiple_of(origin * TOK, TOK), TOK)
        xf[rows, :] = mm(tokF[rows, :], whead[...])

    ready = [sp]
    after = {0: 0, 2: 1, 3: 2, 5: 3, 7: 4, 8: 5, 10: 6}
    for k in range(15):
        for d in range(2):
            tok_wait(d, k)
            if k + 2 < 14:
                tok_send(d, k + 2)
            elif k + 2 == 14:
                if d == 0:
                    tok_send(d, k + 2)
            elif k == 13:
                if d == 1:
                    tok_send(1, 14)
            if k % 2 == 1:
                ready.append(spot(place - (k // 2 + 1), core) if d == 0 else spot(place + (k // 2 + 1), core))
        if k in after:
            j = after[k]
            for d in range(2):
                w_wait(d, j)
                if j + 2 < 6:
                    w_send(d, j + 2)
                elif j == 4 and d == 0:
                    w_send(0, 6)
                elif j == 5 and d == 1:
                    w_send(1, 6)
                mate_send(d, j)
        if k == 0:
            vg_send()
        if k == 8:
            vg_wait()
        if k == 10:
            for m in range(2):
                mate_wait(m, -1)
            for j in range(7):
                for d in range(2):
                    mate_wait(d, j)
            make_head()
        if k > 10:
            for _ in range(min(4, len(ready))):
                project(ready.pop(0))
    ready.append(spot(place - 8, core))
    for origin in ready:
        project(origin)

    def turn_all(i, _):
        cols = pl.ds(pl.multiple_of(i * 256, 256), 256)
        xt = rot_t(xf[cols, :].T, cosT[:, cols], sinT[:, cols], 1.0)
        rotT[:, cols] = xt.astype(BF16)
        rot[cols, :] = xt.T.astype(BF16)
        return 0
    lax.fori_loop(0, SEQ // 256, turn_all, 0)

    attention(lam_ref[sp], rot, rotT, vgF, vgT, cosT, sinT, dqT, acc, e1, e2, mix, dp)

    def fin(i, _):
        cols = pl.ds(pl.multiple_of(i * 256, 256), 256)
        kvT = acc[cols, :].T
        c, s = cosT[:, cols], sinT[:, cols]
        bt = jnp.concatenate([rot_t(dqT[:, cols], c, s, -1.0), rot_t(kvT[0:64], c, s, -1.0)], axis=0)
        backT[:, cols] = bt.astype(BF16)
        xf[cols, :] = bt.T
        return 0
    lax.fori_loop(0, SEQ // 256, fin, 0)

    def pack(i, _):
        r = pl.multiple_of(i * TOK, TOK)
        bpack[i, 0:TOK, :] = xf[pl.ds(r, TOK), :].astype(BF16)
        dv0 = acc[pl.ds(r, HALF), :]
        dv1 = acc[pl.ds(r + HALF, HALF), :]
        bpack[i, TOK:TOK + HALF, :] = jnp.concatenate([dv0[:, 64:], dv1[:, 64:]], axis=1).astype(BF16)
        return 0
    lax.fori_loop(0, 16, pack, 0)
    bF[sp] = bpack[sp]

    def dw(i, _):
        cols = pl.ds(pl.multiple_of(i * 256, 256), 256)
        r = mm(backT[...], tokF[:, cols]).astype(BF16)
        dwp[2 * i] = r[:, :128]
        dwp[2 * i + 1] = r[:, 128:]
        return 0
    lax.fori_loop(0, 8, dw, 0)

    for d in range(1, 16):
        to = lax.rem(sp + d, 16)
        send(bpack.at[to], bF.at[sp], bsend.at[d], brecv.at[d], {"sp": to})
    for d in range(1, 16):
        to = lax.rem(dpi + d, 16)
        send(dwp.at[to], dwR.at[dpi], rsend.at[d], rrecv.at[d], {"dp": to})
    dwR[dpi] = dwp[dpi]

    for d in range(1, 16):
        arrive(dwR.at[lax.rem(dpi + 16 - d, 16)], rsend.at[d], rrecv.at[d])
    total = dwR[0].astype(F32)
    for i in range(1, 16):
        total += dwR[i].astype(F32)
    dwS[...] = total.T.astype(BF16)
    dwG[sp] = total.T.astype(BF16)
    for d in range(1, 16):
        arrive(bF.at[lax.rem(sp + 16 - d, 16)], bsend.at[d], brecv.at[d])
    for d in range(1, 16):
        send(dwS, dwG.at[sp], gsend.at[d], grecv.at[d], {"sp": lax.rem(sp + d, 16)})

    bq, bk = [], []
    for p in range(8):
        lanes = slice(p * 128, (p + 1) * 128)
        a, b = bF[2 * p], bF[2 * p + 1]
        q, k = join(a[:TOK], b[:TOK])
        bq.append(q)
        bk.append(k)
        top, low = join(a[TOK:], b[TOK:])
        vgrad_ref[0:HALF, lanes] = top
        vgrad_ref[HALF:TOK, lanes] = low
    bq = jnp.concatenate(bq, axis=1)
    bk = jnp.concatenate(bk, axis=1)
    for n in range(8):
        rows = slice(n * 256, (n + 1) * 256)
        tg_ref[:, rows] = (mm(bq, wqF[rows, :], TRANS_B) + mm(bk, wkF[rows, :], TRANS_B)).astype(BF16)

    for d in range(1, 16):
        arrive(dwG.at[lax.rem(sp + 16 - d, 16)], gsend.at[d], grecv.at[d])
    for p in range(8):
        lanes = slice(p * 128, (p + 1) * 128)
        q, k = join(dwG[2 * p].astype(F32), dwG[2 * p + 1].astype(F32))
        dwq_ref[:, lanes] = q * factor
        dwk_ref[:, lanes] = k * factor
    for c in sends:
        c.wait_send()


def body(tokens, query_weight, key_weight, values, lambdas, out_grad):
    half = DQK // 2
    freqs = jnp.exp(-math.log(THETA) * jnp.arange(half, dtype=F32) / half)
    angles = freqs[:, None] * jnp.arange(SEQ, dtype=jnp.int32).astype(F32)[None, :]
    vm = pl.BlockSpec(memory_space=pltpu.VMEM)
    dma = pltpu.SemaphoreType.DMA
    V = pltpu.VMEM
    return_shapes = (
        jax.ShapeDtypeStruct((TOK, D), BF16),
        jax.ShapeDtypeStruct((TOK, COLS), BF16),
        jax.ShapeDtypeStruct((128, COLS), F32),
        jax.ShapeDtypeStruct((128, COLS), F32),
    )
    import functools
    tg, vg, dq, dk = pl.pallas_call(
        functools.partial(kernel, 1.0 / math.sqrt(16 * SEQ)),
        out_shape=return_shapes,
        in_specs=[pl.BlockSpec(memory_space=pltpu.SMEM)] + [vm] * 7,
        out_specs=(vm,) * 4,
        scratch_shapes=[
            V((SEQ, D), BF16), V((D, COLS), BF16), V((D, COLS), BF16), V((D, 128), BF16), V((SEQ, 128), F32),
            V((16, TOK, 128), BF16), V((SEQ, 128), BF16),
            V((SEQ, 128), BF16), V((128, SEQ), BF16), V((128, SEQ), BF16), V((64, SEQ), F32), V((SEQ, 128), F32),
            V((SEQ, BQ), F32), V((SEQ, BQ), F32), V((SEQ, BQ), BF16), V((SEQ, BQ), F32),
            V((128, SEQ), BF16), V((16, TOK + HALF, 128), BF16), V((16, TOK + HALF, 128), BF16),
            V((16, 128, 128), BF16), V((16, 128, 128), BF16), V((128, 128), BF16), V((16, 128, 128), BF16),
            dma((2, 15)), dma((2, 15)), dma((2, 7)), dma((2, 7)), dma((16,)), dma((16,)), dma((16,)), dma((16,)),
            dma((16,)), dma((16,)), dma((16,)), dma((16,)), dma((16,)), dma((16,)), dma((3,)),
        ],
        compiler_params=pltpu.CompilerParams(vmem_limit_bytes=60 * 1024 * 1024, collective_id=0, has_side_effects=True),
        name="differential_backward",
    )(lambdas, tokens[0], query_weight, key_weight, values[0], out_grad[0], jnp.cos(angles), jnp.sin(angles))
    return tg[None], vg[None], dq, dk


def solution(mesh):
    in_specs = (
        P("dp", "sp", None),
        P("dp", None),
        P("dp", None),
        P("dp", "sp", None),
        P(),
        P("dp", "sp", None),
    )
    out_specs = (P("dp", "sp", None), P("dp", "sp", None), P("dp", None), P("dp", None))
    return jax.shard_map(body, mesh=mesh, in_specs=in_specs, out_specs=out_specs, check_vma=False)
```

```python
import functools
import math

import jax
import jax.numpy as jnp
from jax import lax
from jax.experimental import pallas as pl
from jax.experimental.pallas import tpu as pltpu
from jax.sharding import PartitionSpec as P

THETA = 10000.0
DQK = 32
NORM_EPS = 0.1
F32, BF16 = jnp.float32, jnp.bfloat16
SEQ = 2560
BQ = 256
BK = 512
NB = SEQ // BQ


def mm(a, b, dims=(((1,), (0,)), ((), ()))):
    return lax.dot_general(a, b, dims, preferred_element_type=F32)


def rot_t(x, c, s, sign):
    parts = []
    for base in range(0, x.shape[0], 32):
        a, b = x[base:base + 16], x[base + 16:base + 32]
        parts += [a * c - b * (sign * s), b * c + a * (sign * s)]
    return jnp.concatenate(parts, axis=0)


def fold(x, op):
    r = x.reshape(x.shape[0] // 8, 8, x.shape[1])
    return op(r, axis=0)


def attention(lam, rot_ref, rotT_ref, vg_ref, vgT_ref, cosT, sinT, dqT_ref, acc_ref, e1_ref, e2_ref, mix_ref, dp_ref, hook):
    inv_root = 1.0 / math.sqrt(32)
    c2 = inv_root * math.log2(math.e)
    acc_ref[...] = jnp.zeros_like(acc_ref)
    zq = jnp.zeros((32, BQ), BF16)

    def block(step, _):
        hook(step)
        b = NB - 1 - step
        qs = pl.multiple_of(b * BQ, BQ)
        qcols = pl.ds(qs, BQ)
        last = b // 2
        q1T = rotT_ref[0:32, qcols]
        q2T = rotT_ref[32:64, qcols]
        rhs1 = jnp.concatenate([zq, zq, q1T, zq], axis=0)
        rhs2 = jnp.concatenate([zq, zq, zq, q2T], axis=0)

        def scores(j):
            ks = pl.multiple_of(j * BK, BK)
            kk = rot_ref[pl.ds(ks, BK), :]
            return ks, mm(kk, rhs1), mm(kk, rhs2)

        def ph1(j, c):
            m1, m2 = c
            ks, s1, s2 = scores(j)
            e1_ref[pl.ds(ks, BK), :] = s1
            e2_ref[pl.ds(ks, BK), :] = s2
            return jnp.maximum(m1, fold(s1, jnp.max)), jnp.maximum(m2, fold(s2, jnp.max))

        neg = jnp.full((8, BQ), -jnp.inf, F32)
        m1, m2 = lax.fori_loop(0, last, ph1, (neg, neg))
        ks, s1, s2 = scores(last)
        mask = (ks + lax.broadcasted_iota(jnp.int32, (BK, BQ), 0)) <= (qs + lax.broadcasted_iota(jnp.int32, (BK, BQ), 1))
        s1 = jnp.where(mask, s1, -jnp.inf)
        s2 = jnp.where(mask, s2, -jnp.inf)
        e1_ref[pl.ds(ks, BK), :] = s1
        e2_ref[pl.ds(ks, BK), :] = s2
        m1 = jnp.max(jnp.maximum(m1, fold(s1, jnp.max)), axis=0, keepdims=True)
        m2 = jnp.max(jnp.maximum(m2, fold(s2, jnp.max)), axis=0, keepdims=True)

        def ph2(j, c):
            l1, l2 = c
            rows = pl.ds(pl.multiple_of(j * BK, BK), BK)
            e1 = jnp.exp2((e1_ref[rows, :] - m1) * c2)
            e2 = jnp.exp2((e2_ref[rows, :] - m2) * c2)
            e1_ref[rows, :] = e1
            e2_ref[rows, :] = e2
            return l1 + fold(e1, jnp.sum), l2 + fold(e2, jnp.sum)

        zero = jnp.zeros((8, BQ), F32)
        l1, l2 = lax.fori_loop(0, last + 1, ph2, (zero, zero))
        r1 = 1.0 / jnp.sum(l1, axis=0, keepdims=True)
        r2 = lam / jnp.sum(l2, axis=0, keepdims=True)

        def ph3(j, o):
            rows = pl.ds(pl.multiple_of(j * BK, BK), BK)
            mix = (e1_ref[rows, :] * r1 - e2_ref[rows, :] * r2).astype(BF16)
            mix_ref[rows, :] = mix
            return o + mm(vgT_ref[0:64, rows], mix)

        o = lax.fori_loop(0, last + 1, ph3, jnp.zeros((64, BQ), F32))
        g = vgT_ref[64:128, qcols].astype(F32)
        ns = lax.rsqrt(jnp.mean(o * o, axis=0, keepdims=True) + NORM_EPS)
        ob = ns * g - ns * ns * ns * o * jnp.mean(g * o, axis=0, keepdims=True)
        obT = ob.astype(BF16)
        obp = jnp.concatenate([jnp.zeros((64, BQ), F32), ob], axis=0).T.astype(BF16)
        obz = jnp.concatenate([obT, jnp.zeros((64, BQ), BF16)], axis=0)

        def ph4(j, c):
            d1, d2 = c
            rows = pl.ds(pl.multiple_of(j * BK, BK), BK)
            dp = mm(vg_ref[rows, :], obz)
            dp_ref[rows, :] = dp
            return d1 + fold(dp * e1_ref[rows, :], jnp.sum), d2 + fold(dp * e2_ref[rows, :], jnp.sum)

        d1, d2 = lax.fori_loop(0, last + 1, ph4, (zero, zero))
        r2n = -r2
        d1 = jnp.sum(d1, axis=0, keepdims=True) * r1
        d2 = jnp.sum(d2, axis=0, keepdims=True) * (1.0 / jnp.sum(l2, axis=0, keepdims=True))
        f1 = r1 * inv_root
        f2 = r2n * inv_root
        lane = lax.broadcasted_iota(jnp.int32, (BQ, 128), 1)
        qrows = rot_ref[qcols, :]
        zb = jnp.zeros_like(qrows)
        rhs = jnp.concatenate([jnp.where(lane < 32, qrows, zb), jnp.where((lane >= 32) & (lane < 64), qrows, zb), obp], axis=0)

        def ph5(j, c):
            a1, a2 = c
            rows = pl.ds(pl.multiple_of(j * BK, BK), BK)
            dp = dp_ref[rows, :]
            g1 = (e1_ref[rows, :] * f1 * (dp - d1)).astype(BF16)
            g2 = (e2_ref[rows, :] * f2 * (dp - d2)).astype(BF16)
            lhs = jnp.concatenate([g1, g2, mix_ref[rows, :]], axis=1)
            acc_ref[rows, :] += mm(lhs, rhs)
            return a1 + mm(rotT_ref[64:96, rows], g1), a2 + mm(rotT_ref[96:128, rows], g2)

        za = jnp.zeros((32, BQ), F32)
        a1, a2 = lax.fori_loop(0, last + 1, ph5, (za, za))
        dqT_ref[0:32, qcols] = a1
        dqT_ref[32:64, qcols] = a2
        return 0

    lax.fori_loop(0, NB, block, 0)


TOK = 160
HALF = 80
D = 2048
COLS = 1024
TRANS_B = (((1,), (1,)), ((), ()))
MESH = pl.DeviceIdType.MESH


def join(a, b):
    return jnp.concatenate([a[:, :64], b[:, :64]], axis=1), jnp.concatenate([a[:, 64:], b[:, 64:]], axis=1)


def kernel(factor, lam_ref, tok_ref, wq_ref, wk_ref, v_ref, g_ref, cosT, sinT,
           tg_ref, vgrad_ref, dwq_ref, dwk_ref,
           tokF, wqF, wkF, wh4, wpk, tabC, tabS, qkS, xf, vgpack, vgF, rot, rotT, vgT, dqT, acc, e1, e2, mix, dp,
           backT, bpack, bF, dwp, dwR, dwS, dwG,
           t1s, t1r, t2s, t2r, p1s, p1r, m1s, m1r, hs, hr, qs, qr,
           wsend, wrecv, psend, precv, asend, arecv, bsend, brecv, rsend, rrecv, gsend, grecv, lsem):
    sp = lax.axis_index("sp")
    dpi = lax.axis_index("dp")
    core = lax.rem(dpi, 2)
    z = lax.div(dpi, 2)
    mate = z * 2 + 1 - core
    y, x = lax.div(sp, 4), lax.rem(sp, 4)
    u = y * (1 - core) + x * core
    w = x * (1 - core) + y * core

    def spot(uu, ww):
        uu, ww = lax.rem(uu + 4, 4), lax.rem(ww + 4, 4)
        return 4 * (uu * (1 - core) + ww * core) + ww * (1 - core) + uu * core

    barrier = pltpu.get_barrier_semaphore()
    for d in range(1, 16):
        pl.semaphore_signal(barrier, inc=1, device_id={"sp": lax.rem(sp + d, 16)}, device_id_type=MESH)
        pl.semaphore_signal(barrier, inc=1, device_id={"dp": lax.rem(dpi + d, 16)}, device_id_type=MESH)

    pair = pl.ds(pl.multiple_of(lax.div(sp, 2) * 128, 128), 128)
    lo, hi = join(wq_ref[:, pair], wk_ref[:, pair])
    wpk[...] = jnp.where(lax.rem(sp, 2) == 0, lo, hi)

    for p in range(8):
        lanes = slice(p * 128, (p + 1) * 128)
        vgpack[2 * p], vgpack[2 * p + 1] = join(v_ref[:, lanes], g_ref[:, lanes])

    pl.semaphore_wait(barrier, 30)

    sends = []

    def send(src, dst, ss, rs, to):
        def make():
            return pltpu.make_async_remote_copy(src_ref=src(), dst_ref=dst(), send_sem=ss(), recv_sem=rs(), device_id=to(),
                                                device_id_type=MESH)
        make().start()
        sends.append(make)

    def arrive(dst, ss, rs):
        pltpu.make_async_remote_copy(src_ref=dst, dst_ref=dst, send_sem=ss, recv_sem=rs, device_id={"sp": sp},
                                     device_id_type=MESH).wait_recv()

    def rows_of(i, n, at=0, size=None):
        return pl.ds(pl.multiple_of(i * n + at, 16), size or n)

    def t1_go(d):
        return {"sp": spot(u, w + 1 - 2 * d)}

    def t1_part(d, i):
        back = 1 if i < 2 else 2
        half = d if i != 1 else 1 - d
        return rows_of(spot(u, w - back if d == 0 else w + back), TOK, half * HALF, HALF)

    def t1_send(d, i):
        if i < 2:
            half = d if i == 0 else 1 - d
            send(lambda: tok_ref.at[pl.ds(half * HALF, HALF)], lambda: tokF.at[rows_of(sp, TOK, half * HALF, HALF)],
                 lambda: t1s.at[d, i], lambda: t1r.at[d, i], lambda: t1_go(d))
        else:
            send(lambda: tokF.at[t1_part(d, 0)], lambda: tokF.at[t1_part(d, 0)], lambda: t1s.at[d, i], lambda: t1r.at[d, i], lambda: t1_go(d))

    def t1_wait(d, i):
        arrive(tokF.at[t1_part(d, i)], t1s.at[d, i], t1r.at[d, i])

    def t2_go(d):
        return {"sp": spot(u + 1 - 2 * d, w)}

    def t2_rows(d, back, i, whole):
        b = spot(u - back if d == 0 else u + back, w + i)
        return rows_of(b, TOK) if whole else rows_of(b, TOK, d * HALF, HALF)

    def t2_send(d, i):
        send(lambda: tokF.at[t2_rows(d, 0, i, True)], lambda: tokF.at[t2_rows(d, 0, i, True)],
             lambda: t2s.at[d, i], lambda: t2r.at[d, i], lambda: t2_go(d))

    def t2_event(i):
        for d in range(2):
            arrive(tokF.at[t2_rows(d, 1, i, True)], t2s.at[d, i], t2r.at[d, i])
            send(lambda d=d: tokF.at[t2_rows(d, 1, i, False)], lambda d=d: tokF.at[t2_rows(d, 1, i, False)],
                 lambda d=d: t2s.at[d, 4 + i], lambda d=d: t2r.at[d, 4 + i], lambda d=d: t2_go(d))

    def t2_end():
        for i in range(4):
            for d in range(2):
                arrive(tokF.at[t2_rows(d, 2, i, False)], t2s.at[d, 4 + i], t2r.at[d, 4 + i])

    def lane_block(i):
        return pl.ds(pl.multiple_of(i * 128, 128), 128)

    def p1_send():
        for d in range(1, 8):
            send(lambda: wpk, lambda: wh4.at[rows_of(dpi, 128), lane_block(u)], lambda d=d: p1s.at[d], lambda d=d: p1r.at[d],
                 lambda d=d: {"dp": lax.rem(z + d, 8) * 2 + core})
        send(lambda: wpk, lambda: wh4.at[rows_of(dpi, 128), lane_block(w)], lambda: m1s.at[0], lambda: m1r.at[0], lambda: {"dp": mate})

    def p1_wait():
        for d in (1, 7, 2, 6, 3, 5, 4):
            part = lambda d=d: wh4.at[rows_of(lax.rem(z + 8 - d, 8) * 2 + core, 128), lane_block(u)]
            to = lambda d=d: wh4.at[rows_of(lax.rem(z + 8 - d, 8) * 2 + core, 128), lane_block(w)]
            arrive(part(), p1s.at[d], p1r.at[d])
            send(part, to, lambda d=d: m1s.at[d], lambda d=d: m1r.at[d], lambda: {"dp": mate})
        for d in range(8):
            arrive(wh4.at[rows_of(lax.rem(z + 8 - d, 8) * 2 + 1 - core, 128), lane_block(u)], m1s.at[d], m1r.at[d])

    def h_part(back, d, half):
        return wh4.at[pl.ds(half * 1024, 1024), lane_block(lax.rem(u + 4 - back if d == 0 else u + back, 4))]

    def h_send(d, i):
        half = d if i != 1 else 1 - d
        part = lambda: h_part(0 if i < 2 else 1, d, half)
        send(part, part, lambda: hs.at[d, i], lambda: hr.at[d, i], lambda: t2_go(d))

    def h_wait(d, i):
        arrive(h_part(1 if i < 2 else 2, d, d if i != 1 else 1 - d), hs.at[d, i], hr.at[d, i])

    wF = (wqF, wkF)
    wown = (wq_ref, wk_ref)

    def w_go(d):
        return {"dp": lax.rem(z + 1 + 6 * d, 8) * 2 + core}

    def w_owner(back, d):
        return lax.rem(z + 8 - back if d == 0 else z + back, 8) * 2 + core

    def w_which(d, k):
        return d if k == 6 else k % 2

    def w_send(d, k):
        m = w_which(d, k)
        send(lambda: wown[m] if k < 2 else wF[m].at[rows_of(w_owner(k // 2, d), 128)], lambda: wF[m].at[rows_of(w_owner(k // 2, d), 128)],
             lambda: wsend.at[d, k], lambda: wrecv.at[d, k], lambda: w_go(d))

    def mate_own(m):
        send(lambda: wown[m], lambda: wF[m].at[rows_of(dpi, 128)], lambda: psend.at[14 + m], lambda: precv.at[14 + m], lambda: {"dp": mate})

    def w_event(k):
        for d in range(2):
            m = w_which(d, k)
            part = lambda m=m, d=d: wF[m].at[rows_of(w_owner(k // 2 + 1, d), 128)]
            arrive(part(), wsend.at[d, k], wrecv.at[d, k])
            if k < 4 or k == 4 + d:
                w_send(d, k + 2 if k < 4 else 6)
            send(part, part, lambda d=d: psend.at[d * 7 + k], lambda d=d: precv.at[d * 7 + k], lambda: {"dp": mate})

    def mate_end():
        for m in range(2):
            arrive(wF[m].at[rows_of(mate, 128)], psend.at[14 + m], precv.at[14 + m])
        for k in range(7):
            for d in range(2):
                arrive(wF[w_which(d, k)].at[rows_of(w_owner(k // 2 + 1, d) + 1 - 2 * core, 128)], psend.at[d * 7 + k], precv.at[d * 7 + k])

    def vg_send():
        for d in range(1, 16):
            send(lambda d=d: vgpack.at[lax.rem(sp + d, 16)], lambda: vgF.at[rows_of(sp, TOK)], lambda d=d: asend.at[d], lambda d=d: arecv.at[d],
                 lambda d=d: {"sp": lax.rem(sp + d, 16)})

    def vg_wait():
        for d in range(1, 16):
            arrive(vgF.at[rows_of(lax.rem(sp + 16 - d, 16), TOK)], asend.at[d], arecv.at[d])

    def qk_send():
        for du in range(1, 4):
            for i in range(4):
                send(lambda du=du, i=i: qkS.at[lax.rem(u + du, 4), i], lambda i=i: rot.at[rows_of(spot(u, w + i), TOK)],
                     lambda du=du, i=i: qs.at[du, i], lambda du=du, i=i: qr.at[du, i], lambda du=du: {"sp": spot(u + du, w)})

    def qk_wait():
        for du in range(1, 4):
            for i in range(4):
                arrive(rot.at[rows_of(spot(u - du, w + i), TOK)], qs.at[du, i], qr.at[du, i])

    for i in range(2):
        for d in range(2):
            t1_send(d, i)
    p1_send()
    own = [pltpu.make_async_copy(tok_ref, tokF.at[rows_of(sp, TOK)], lsem.at[0]),
           pltpu.make_async_copy(wq_ref, wqF.at[rows_of(dpi, 128)], lsem.at[1]),
           pltpu.make_async_copy(wk_ref, wkF.at[rows_of(dpi, 128)], lsem.at[2])]
    for c in own:
        c.start()
    wh4[rows_of(dpi, 128), lane_block(u)] = wpk[...]
    vgF[rows_of(sp, TOK), :] = vgpack[sp]

    def tables(i, _):
        cols = pl.ds(pl.multiple_of(i * 128, 128), 128)
        c, s = cosT[:, cols], sinT[:, cols]
        tabC[cols, :] = jnp.concatenate([c] * 8, axis=0).T
        tabS[cols, :] = jnp.concatenate([-s, s] * 4, axis=0).T
        return 0
    lax.fori_loop(0, SEQ // 128, tables, 0)
    for c in own:
        c.wait()

    for d in range(2):
        t1_wait(d, 0)
        t1_send(d, 2)
    p1_wait()
    for i in range(2):
        for d in range(2):
            h_send(d, i)
    for k in range(2):
        for d in range(2):
            w_send(d, k)
    for m in range(2):
        mate_own(m)
    for d in range(2):
        t1_wait(d, 1)
        t1_wait(d, 2)
    for d in range(2):
        h_wait(d, 0)
        h_send(d, 2)
    vg_send()
    for d in range(2):
        h_wait(d, 1)
        h_wait(d, 2)

    lane16 = lax.rem(lax.broadcasted_iota(jnp.int32, (TOK, 128), 1), 32) < 16

    def project(i, _):
        b = spot(u, w + i)
        rows = rows_of(b, TOK)
        r = mm(tokF[rows, :], wh4[...])
        c, s = tabC[rows, :], tabS[rows, :]
        for h in range(4):
            a = r[:, h * 128:(h + 1) * 128]
            other = jnp.where(lane16, pltpu.roll(a, 112, 1), pltpu.roll(a, 16, 1))
            qkS[h, i] = (a * c + other * s).astype(BF16)
        return 0
    lax.fori_loop(0, 4, project, 0)
    for i in range(4):
        rot[rows_of(spot(u, w + i), TOK), :] = qkS[u, i]
    qk_send()
    for i in range(4):
        for d in range(2):
            t2_send(d, i)
    w_event(0)
    w_event(1)
    vg_wait()

    def turn_vg(i, _):
        r = pl.multiple_of(i * 256, 256)
        vgT[:, pl.ds(r, 256)] = vgF[pl.ds(r, 256), :].astype(F32).T.astype(BF16)
        return 0
    lax.fori_loop(0, SEQ // 256, turn_vg, 0)
    w_event(2)
    qk_wait()

    def turn_qk(i, _):
        r = pl.multiple_of(i * 256, 256)
        rotT[:, pl.ds(r, 256)] = rot[pl.ds(r, 256), :].astype(F32).T.astype(BF16)
        return 0
    lax.fori_loop(0, SEQ // 256, turn_qk, 0)

    def hook(step):
        plan = {0: [lambda: w_event(3)], 1: [lambda: t2_event(0), lambda: w_event(4)], 2: [lambda: t2_event(1), lambda: w_event(5)],
                3: [lambda: t2_event(2), lambda: w_event(6)], 4: [lambda: t2_event(3)]}
        for s, jobs in plan.items():
            @pl.when(step == s)
            def _():
                for j in jobs:
                    j()

    attention(lam_ref[sp], rot, rotT, vgF, vgT, cosT, sinT, dqT, acc, e1, e2, mix, dp, hook)

    def fin(i, _):
        cols = pl.ds(pl.multiple_of(i * 256, 256), 256)
        kvT = acc[cols, :].T
        c, s = cosT[:, cols], sinT[:, cols]
        bt = jnp.concatenate([rot_t(dqT[:, cols], c, s, -1.0), rot_t(kvT[0:64], c, s, -1.0)], axis=0)
        backT[:, cols] = bt.astype(BF16)
        xf[cols, :] = bt.T
        return 0
    lax.fori_loop(0, SEQ // 256, fin, 0)

    def pack(i, _):
        r = pl.multiple_of(i * TOK, TOK)
        bpack[i, 0:TOK, :] = xf[pl.ds(r, TOK), :].astype(BF16)
        dv0 = acc[pl.ds(r, HALF), :]
        dv1 = acc[pl.ds(r + HALF, HALF), :]
        bpack[i, TOK:TOK + HALF, :] = jnp.concatenate([dv0[:, 64:], dv1[:, 64:]], axis=1).astype(BF16)
        return 0
    lax.fori_loop(0, 16, pack, 0)
    bF[sp] = bpack[sp]
    t2_end()
    mate_end()

    def dw(i, _):
        cols = pl.ds(pl.multiple_of(i * 256, 256), 256)
        r = mm(backT[...], tokF[:, cols]).astype(BF16)
        dwp[2 * i] = r[:, :128]
        dwp[2 * i + 1] = r[:, 128:]
        return 0
    lax.fori_loop(0, 8, dw, 0)

    for d in range(1, 16):
        send(lambda d=d: bpack.at[lax.rem(sp + d, 16)], lambda: bF.at[sp], lambda d=d: bsend.at[d], lambda d=d: brecv.at[d],
             lambda d=d: {"sp": lax.rem(sp + d, 16)})
    for d in range(1, 16):
        send(lambda d=d: dwp.at[lax.rem(dpi + d, 16)], lambda: dwR.at[dpi], lambda d=d: rsend.at[d], lambda d=d: rrecv.at[d],
             lambda d=d: {"dp": lax.rem(dpi + d, 16)})
    dwR[dpi] = dwp[dpi]

    for d in range(1, 16):
        arrive(dwR.at[lax.rem(dpi + 16 - d, 16)], rsend.at[d], rrecv.at[d])
    total = dwR[0].astype(F32)
    for i in range(1, 16):
        total += dwR[i].astype(F32)
    dwS[...] = total.T.astype(BF16)
    dwG[sp] = total.T.astype(BF16)
    for d in range(1, 16):
        arrive(bF.at[lax.rem(sp + 16 - d, 16)], bsend.at[d], brecv.at[d])
    for d in range(1, 16):
        send(lambda: dwS, lambda: dwG.at[sp], lambda d=d: gsend.at[d], lambda d=d: grecv.at[d], lambda d=d: {"sp": lax.rem(sp + d, 16)})

    bq, bk = [], []
    for p in range(8):
        lanes = slice(p * 128, (p + 1) * 128)
        a, b = bF[2 * p], bF[2 * p + 1]
        q, k = join(a[:TOK], b[:TOK])
        bq.append(q)
        bk.append(k)
        top, low = join(a[TOK:], b[TOK:])
        vgrad_ref[0:HALF, lanes] = top
        vgrad_ref[HALF:TOK, lanes] = low
    bq = jnp.concatenate(bq, axis=1)
    bk = jnp.concatenate(bk, axis=1)
    for n in range(8):
        rows = slice(n * 256, (n + 1) * 256)
        tg_ref[:, rows] = (mm(bq, wqF[rows, :], TRANS_B) + mm(bk, wkF[rows, :], TRANS_B)).astype(BF16)

    for d in range(1, 16):
        arrive(dwG.at[lax.rem(sp + 16 - d, 16)], gsend.at[d], grecv.at[d])
    for p in range(8):
        lanes = slice(p * 128, (p + 1) * 128)
        q, k = join(dwG[2 * p].astype(F32), dwG[2 * p + 1].astype(F32))
        dwq_ref[:, lanes] = q * factor
        dwk_ref[:, lanes] = k * factor
    for make in sends:
        make().wait_send()


def body(tokens, query_weight, key_weight, values, lambdas, out_grad):
    half = DQK // 2
    freqs = jnp.exp(-math.log(THETA) * jnp.arange(half, dtype=F32) / half)
    angles = freqs[:, None] * jnp.arange(SEQ, dtype=jnp.int32).astype(F32)[None, :]
    vm = pl.BlockSpec(memory_space=pltpu.VMEM)
    dma = pltpu.SemaphoreType.DMA
    V = pltpu.VMEM
    return_shapes = (
        jax.ShapeDtypeStruct((TOK, D), BF16),
        jax.ShapeDtypeStruct((TOK, COLS), BF16),
        jax.ShapeDtypeStruct((128, COLS), F32),
        jax.ShapeDtypeStruct((128, COLS), F32),
    )
    tg, vg, dq, dk = pl.pallas_call(
        functools.partial(kernel, 1.0 / math.sqrt(16 * SEQ)),
        out_shape=return_shapes,
        in_specs=[pl.BlockSpec(memory_space=pltpu.SMEM)] + [vm] * 7,
        out_specs=(vm,) * 4,
        scratch_shapes=[
            V((SEQ, D), BF16), V((D, COLS), BF16), V((D, COLS), BF16), V((D, 512), BF16), V((128, 128), BF16),
            V((SEQ, 128), F32), V((SEQ, 128), F32), V((4, 4, TOK, 128), BF16), V((SEQ, 128), F32),
            V((16, TOK, 128), BF16), V((SEQ, 128), BF16),
            V((SEQ, 128), BF16), V((128, SEQ), BF16), V((128, SEQ), BF16), V((64, SEQ), F32), V((SEQ, 128), F32),
            V((SEQ, BQ), F32), V((SEQ, BQ), F32), V((SEQ, BQ), BF16), V((SEQ, BQ), F32),
            V((128, SEQ), BF16), V((16, TOK + HALF, 128), BF16), V((16, TOK + HALF, 128), BF16),
            V((16, 128, 128), BF16), V((16, 128, 128), BF16), V((128, 128), BF16), V((16, 128, 128), BF16),
            dma((2, 3)), dma((2, 3)), dma((2, 8)), dma((2, 8)), dma((8,)), dma((8,)), dma((8,)), dma((8,)),
            dma((2, 3)), dma((2, 3)), dma((4, 4)), dma((4, 4)),
            dma((2, 7)), dma((2, 7)), dma((16,)), dma((16,)), dma((16,)), dma((16,)),
            dma((16,)), dma((16,)), dma((16,)), dma((16,)), dma((16,)), dma((16,)), dma((3,)),
        ],
        compiler_params=pltpu.CompilerParams(vmem_limit_bytes=62 * 1024 * 1024, collective_id=0, has_side_effects=True),
        name="differential_backward",
    )(lambdas, tokens[0], query_weight, key_weight, values[0], out_grad[0], jnp.cos(angles), jnp.sin(angles))
    return tg[None], vg[None], dq, dk


def solution(mesh):
    in_specs = (
        P("dp", "sp", None),
        P("dp", None),
        P("dp", None),
        P("dp", "sp", None),
        P(),
        P("dp", "sp", None),
    )
    out_specs = (P("dp", "sp", None), P("dp", "sp", None), P("dp", None), P("dp", None))
    return jax.shard_map(body, mesh=mesh, in_specs=in_specs, out_specs=out_specs, check_vma=False)
```

```python
import functools
import math

import jax
import jax.numpy as jnp
import numpy as np
from jax import lax
from jax.experimental import pallas as pl
from jax.experimental.pallas import tpu as pltpu
from jax.sharding import PartitionSpec as P

THETA = 10000.0
DQK = 32
NORM_EPS = 0.1
F32, BF16 = jnp.float32, jnp.bfloat16
SEQ = 2560
BQ = 512
BK = 512
NB = SEQ // BQ


def mm(a, b, dims=(((1,), (0,)), ((), ()))):
    return lax.dot_general(a, b, dims, preferred_element_type=F32)


def rot_t(x, c, s, sign):
    parts = []
    for base in range(0, x.shape[0], 32):
        a, b = x[base:base + 16], x[base + 16:base + 32]
        parts += [a * c - b * (sign * s), b * c + a * (sign * s)]
    return jnp.concatenate(parts, axis=0)


def fold(x, op):
    r = x.reshape(x.shape[0] // 8, 8, x.shape[1])
    return op(r, axis=0)


def attention(lam, rot_ref, rotT_ref, vg_ref, vgT_ref, cosT, sinT, dqT_ref, acc_ref, e1_ref, e2_ref, mix_ref, dp_ref, hook, done):
    inv_root = 1.0 / math.sqrt(32)
    c2 = inv_root * math.log2(math.e)
    acc_ref[...] = jnp.zeros_like(acc_ref)
    zq = jnp.zeros((32, BQ), BF16)

    def block(step, _):
        hook(step, 0)
        b = NB - 1 - step
        qs = pl.multiple_of(b * BQ, BQ)
        qcols = pl.ds(qs, BQ)
        last = b
        q1T = rotT_ref[0:32, qcols]
        q2T = rotT_ref[32:64, qcols]
        rhs1 = jnp.concatenate([zq, zq, q1T, zq], axis=0)
        rhs2 = jnp.concatenate([zq, zq, zq, q2T], axis=0)

        def scores(j):
            ks = pl.multiple_of(j * BK, BK)
            kk = rot_ref[pl.ds(ks, BK), :]
            return ks, mm(kk, rhs1), mm(kk, rhs2)

        def ph1(j, c):
            m1, m2 = c
            ks, s1, s2 = scores(j)
            e1_ref[pl.ds(ks, BK), :] = s1
            e2_ref[pl.ds(ks, BK), :] = s2
            return jnp.maximum(m1, fold(s1, jnp.max)), jnp.maximum(m2, fold(s2, jnp.max))

        neg = jnp.full((8, BQ), -jnp.inf, F32)
        m1, m2 = lax.fori_loop(0, last, ph1, (neg, neg))
        ks, s1, s2 = scores(last)
        mask = (ks + lax.broadcasted_iota(jnp.int32, (BK, BQ), 0)) <= (qs + lax.broadcasted_iota(jnp.int32, (BK, BQ), 1))
        s1 = jnp.where(mask, s1, -jnp.inf)
        s2 = jnp.where(mask, s2, -jnp.inf)
        e1_ref[pl.ds(ks, BK), :] = s1
        e2_ref[pl.ds(ks, BK), :] = s2
        m1 = jnp.max(jnp.maximum(m1, fold(s1, jnp.max)), axis=0, keepdims=True)
        m2 = jnp.max(jnp.maximum(m2, fold(s2, jnp.max)), axis=0, keepdims=True)

        def ph2(j, c):
            l1, l2 = c
            rows = pl.ds(pl.multiple_of(j * BK, BK), BK)
            e1 = jnp.exp2((e1_ref[rows, :] - m1) * c2)
            e2 = jnp.exp2((e2_ref[rows, :] - m2) * c2)
            e1_ref[rows, :] = e1
            e2_ref[rows, :] = e2
            return l1 + fold(e1, jnp.sum), l2 + fold(e2, jnp.sum)

        zero = jnp.zeros((8, BQ), F32)
        l1, l2 = lax.fori_loop(0, last + 1, ph2, (zero, zero))
        r1 = 1.0 / jnp.sum(l1, axis=0, keepdims=True)
        r2 = lam / jnp.sum(l2, axis=0, keepdims=True)

        def ph3(j, o):
            rows = pl.ds(pl.multiple_of(j * BK, BK), BK)
            mix = (e1_ref[rows, :] * r1 - e2_ref[rows, :] * r2).astype(BF16)
            mix_ref[rows, :] = mix
            return o + mm(vgT_ref[0:64, rows], mix)

        o = lax.fori_loop(0, last + 1, ph3, jnp.zeros((64, BQ), F32))
        hook(step, 1)
        g = vgT_ref[64:128, qcols].astype(F32)
        ns = lax.rsqrt(jnp.mean(o * o, axis=0, keepdims=True) + NORM_EPS)
        ob = ns * g - ns * ns * ns * o * jnp.mean(g * o, axis=0, keepdims=True)
        obT = ob.astype(BF16)
        obp = jnp.concatenate([jnp.zeros((64, BQ), F32), ob], axis=0).T.astype(BF16)
        obz = jnp.concatenate([obT, jnp.zeros((64, BQ), BF16)], axis=0)

        def ph4(j, c):
            d1, d2 = c
            rows = pl.ds(pl.multiple_of(j * BK, BK), BK)
            dp = mm(vg_ref[rows, :], obz)
            dp_ref[rows, :] = dp
            return d1 + fold(dp * e1_ref[rows, :], jnp.sum), d2 + fold(dp * e2_ref[rows, :], jnp.sum)

        d1, d2 = lax.fori_loop(0, last + 1, ph4, (zero, zero))
        r2n = -r2
        d1 = jnp.sum(d1, axis=0, keepdims=True) * r1
        d2 = jnp.sum(d2, axis=0, keepdims=True) * (1.0 / jnp.sum(l2, axis=0, keepdims=True))
        f1 = r1 * inv_root
        f2 = r2n * inv_root
        lane = lax.broadcasted_iota(jnp.int32, (BQ, 128), 1)
        qrows = rot_ref[qcols, :]
        zb = jnp.zeros_like(qrows)
        rhs = jnp.concatenate([jnp.where(lane < 32, qrows, zb), jnp.where((lane >= 32) & (lane < 64), qrows, zb), obp], axis=0)

        def ph5(j, c):
            a1, a2 = c
            rows = pl.ds(pl.multiple_of(j * BK, BK), BK)
            dp = dp_ref[rows, :]
            g1 = (e1_ref[rows, :] * f1 * (dp - d1)).astype(BF16)
            g2 = (e2_ref[rows, :] * f2 * (dp - d2)).astype(BF16)
            lhs = jnp.concatenate([g1, g2, mix_ref[rows, :]], axis=1)
            acc_ref[rows, :] += mm(lhs, rhs)
            return a1 + mm(rotT_ref[64:96, rows], g1), a2 + mm(rotT_ref[96:128, rows], g2)

        za = jnp.zeros((32, BQ), F32)
        a1, a2 = lax.fori_loop(0, last + 1, ph5, (za, za))
        dqT_ref[0:32, qcols] = a1
        dqT_ref[32:64, qcols] = a2
        done(step, b)
        return 0

    lax.fori_loop(0, NB, block, 0)


TOK = 160
HALF = 80
D = 2048
COLS = 1024
TRANS_B = (((1,), (1,)), ((), ()))
MESH = pl.DeviceIdType.MESH


def join(a, b):
    return jnp.concatenate([a[:, :64], b[:, :64]], axis=1), jnp.concatenate([a[:, 64:], b[:, 64:]], axis=1)


def kernel(lam_ref, tok_ref, wq_ref, wk_ref, v_ref, g_ref, cosT, sinT,
           tg_ref, vgrad_ref, dw_ref,
           tokF, wqF, wkF, wh4, wpk, tabC, tabS, qkS, xf, vgpack, vgF, rot, rotT, vgT, dqT, acc, e1, e2, mix, dp,
           backT, bpack, bF, dwp, dwM, dwP, dwR, dwS, dwG,
           t1s, t1r, t2s, t2r, p1s, p1r, m1s, m1r, hs, hr, qs, qr,
           wsend, wrecv, psend, precv, asend, arecv, bsend, brecv, rsend, rrecv, gsend, grecv, lsem):
    sp = lax.axis_index("sp")
    dpi = lax.axis_index("dp")
    core = lax.rem(dpi, 2)
    z = lax.div(dpi, 2)
    mate = z * 2 + 1 - core
    y, x = lax.div(sp, 4), lax.rem(sp, 4)
    u = y * (1 - core) + x * core
    w = x * (1 - core) + y * core

    def spot(uu, ww):
        uu, ww = lax.rem(uu + 4, 4), lax.rem(ww + 4, 4)
        return 4 * (uu * (1 - core) + ww * core) + ww * (1 - core) + uu * core

    barrier = pltpu.get_barrier_semaphore()
    for d in range(1, 16):
        pl.semaphore_signal(barrier, inc=1, device_id={"sp": lax.rem(sp + d, 16)}, device_id_type=MESH)
        pl.semaphore_signal(barrier, inc=1, device_id={"dp": lax.rem(dpi + d, 16)}, device_id_type=MESH)

    pair = pl.ds(pl.multiple_of(lax.div(sp, 2) * 128, 128), 128)
    lo, hi = join(wq_ref[:, pair], wk_ref[:, pair])
    wpk[...] = jnp.where(lax.rem(sp, 2) == 0, lo, hi)

    for p in range(8):
        lanes = slice(p * 128, (p + 1) * 128)
        vgpack[2 * p], vgpack[2 * p + 1] = join(v_ref[:, lanes], g_ref[:, lanes])

    pl.semaphore_wait(barrier, 30)

    sends = []

    def send(src, dst, ss, rs, to, when=None):
        def make():
            return pltpu.make_async_remote_copy(src_ref=src(), dst_ref=dst(), send_sem=ss(), recv_sem=rs(), device_id=to(),
                                                device_id_type=MESH)
        make().start()
        sends.append((make, when))

    def arrive(dst, ss, rs):
        pltpu.make_async_remote_copy(src_ref=dst, dst_ref=dst, send_sem=ss, recv_sem=rs, device_id={"sp": sp},
                                     device_id_type=MESH).wait_recv()

    def rows_of(i, n, at=0, size=None):
        return pl.ds(pl.multiple_of(i * n + at, 16), size or n)

    def t1_go(d):
        return {"sp": spot(u, w + 1 - 2 * d)}

    def t1_part(d, i):
        back = 1 if i < 2 else 2
        half = d if i != 1 else 1 - d
        return rows_of(spot(u, w - back if d == 0 else w + back), TOK, half * HALF, HALF)

    def t1_send(d, i):
        if i < 2:
            half = d if i == 0 else 1 - d
            send(lambda: tok_ref.at[pl.ds(half * HALF, HALF)], lambda: tokF.at[rows_of(sp, TOK, half * HALF, HALF)],
                 lambda: t1s.at[d, i], lambda: t1r.at[d, i], lambda: t1_go(d))
        else:
            send(lambda: tokF.at[t1_part(d, 0)], lambda: tokF.at[t1_part(d, 0)], lambda: t1s.at[d, i], lambda: t1r.at[d, i], lambda: t1_go(d))

    def t1_wait(d, i):
        arrive(tokF.at[t1_part(d, i)], t1s.at[d, i], t1r.at[d, i])

    def t2_go(d):
        return {"sp": spot(u + 1 - 2 * d, w)}

    def t2_rows(d, back, i, half):
        return rows_of(spot(u - back if d == 0 else u + back, w + i), TOK, half * HALF, HALF)

    def t2_send(d, i, k):
        half = d if k != 1 else 1 - d
        part = lambda: tokF.at[t2_rows(d, 1 if k == 2 else 0, i, half)]
        src = (lambda: tok_ref.at[pl.ds(half * HALF, HALF)]) if i == 0 and k < 2 else part
        send(src, part, lambda: t2s.at[d, i, k], lambda: t2r.at[d, i, k], lambda: t2_go(d))

    def t2_wait(d, i, k):
        arrive(tokF.at[t2_rows(d, 2 if k == 2 else 1, i, d if k != 1 else 1 - d)], t2s.at[d, i, k], t2r.at[d, i, k])

    def t2_event(i):
        for d in range(2):
            t2_wait(d, i, 0)
            t2_send(d, i, 2)

    def t2_end():
        for i in range(4):
            for d in range(2):
                t2_wait(d, i, 1)
                t2_wait(d, i, 2)

    def lane_block(i):
        return pl.ds(pl.multiple_of(i * 128, 128), 128)

    def p1_send():
        for d in range(1, 8):
            send(lambda: wpk, lambda: wh4.at[rows_of(dpi, 128), lane_block(u)], lambda d=d: p1s.at[d], lambda d=d: p1r.at[d],
                 lambda d=d: {"dp": lax.rem(z + d, 8) * 2 + core})
        send(lambda: wpk, lambda: wh4.at[rows_of(dpi, 128), lane_block(w)], lambda: m1s.at[0], lambda: m1r.at[0], lambda: {"dp": mate})

    def p1_wait():
        for d in (1, 7, 2, 6, 3, 5, 4):
            part = lambda d=d: wh4.at[rows_of(lax.rem(z + 8 - d, 8) * 2 + core, 128), lane_block(u)]
            to = lambda d=d: wh4.at[rows_of(lax.rem(z + 8 - d, 8) * 2 + core, 128), lane_block(w)]
            arrive(part(), p1s.at[d], p1r.at[d])
            send(part, to, lambda d=d: m1s.at[d], lambda d=d: m1r.at[d], lambda: {"dp": mate})
        for d in range(8):
            arrive(wh4.at[rows_of(lax.rem(z + 8 - d, 8) * 2 + 1 - core, 128), lane_block(u)], m1s.at[d], m1r.at[d])

    def h_part(back, d, half):
        return wh4.at[pl.ds(half * 1024, 1024), lane_block(lax.rem(u + 4 - back if d == 0 else u + back, 4))]

    def h_send(d, i):
        half = d if i != 1 else 1 - d
        part = lambda: h_part(0 if i < 2 else 1, d, half)
        send(part, part, lambda: hs.at[d, i], lambda: hr.at[d, i], lambda: t2_go(d))

    def h_wait(d, i):
        arrive(h_part(1 if i < 2 else 2, d, d if i != 1 else 1 - d), hs.at[d, i], hr.at[d, i])

    wF = (wqF, wkF)
    wown = (wq_ref, wk_ref)

    def w_go(d):
        return {"dp": lax.rem(z + 1 + 6 * d, 8) * 2 + core}

    def w_owner(back, d):
        return lax.rem(z + 8 - back if d == 0 else z + back, 8) * 2 + core

    def w_which(d, k):
        return d if k == 6 else k % 2

    def w_send(d, k):
        m = w_which(d, k)
        send(lambda: wown[m] if k < 2 else wF[m].at[rows_of(w_owner(k // 2, d), 128)], lambda: wF[m].at[rows_of(w_owner(k // 2, d), 128)],
             lambda: wsend.at[d, k], lambda: wrecv.at[d, k], lambda: w_go(d))

    def mate_own(m):
        send(lambda: wown[m], lambda: wF[m].at[rows_of(dpi, 128)], lambda: psend.at[14 + m], lambda: precv.at[14 + m], lambda: {"dp": mate})

    def w_event(k):
        for d in range(2):
            m = w_which(d, k)
            part = lambda m=m, d=d: wF[m].at[rows_of(w_owner(k // 2 + 1, d), 128)]
            arrive(part(), wsend.at[d, k], wrecv.at[d, k])
            if k < 4 or k == 4 + d:
                w_send(d, k + 2 if k < 4 else 6)
            send(part, part, lambda d=d: psend.at[d * 7 + k], lambda d=d: precv.at[d * 7 + k], lambda: {"dp": mate})

    def mate_end():
        for m in range(2):
            arrive(wF[m].at[rows_of(mate, 128)], psend.at[14 + m], precv.at[14 + m])
        for k in range(7):
            for d in range(2):
                arrive(wF[w_which(d, k)].at[rows_of(w_owner(k // 2 + 1, d) + 1 - 2 * core, 128)], psend.at[d * 7 + k], precv.at[d * 7 + k])

    def vg_send():
        for d in range(1, 16):
            send(lambda d=d: vgpack.at[lax.rem(sp + d, 16)], lambda: vgF.at[rows_of(sp, TOK)], lambda d=d: asend.at[d], lambda d=d: arecv.at[d],
                 lambda d=d: {"sp": lax.rem(sp + d, 16)})

    def vg_wait():
        for d in range(1, 16):
            arrive(vgF.at[rows_of(lax.rem(sp + 16 - d, 16), TOK)], asend.at[d], arecv.at[d])

    def qk_send(i):
        for du in (1, 3, 2):
            send(lambda du=du: qkS.at[lax.rem(u + du, 4), i], lambda: rot.at[rows_of(spot(u, w + i), TOK)],
                 lambda du=du: qs.at[du, i], lambda du=du: qr.at[du, i], lambda du=du: {"sp": spot(u + du, w)})

    def qk_wait():
        for du in range(1, 4):
            for i in range(4):
                arrive(rot.at[rows_of(spot(u - du, w + i), TOK)], qs.at[du, i], qr.at[du, i])

    for i in range(2):
        for d in range(2):
            t1_send(d, i)
    p1_send()
    for d in range(2):
        t2_send(d, 0, 0)
    own = [pltpu.make_async_copy(tok_ref, tokF.at[rows_of(sp, TOK)], lsem.at[0]),
           pltpu.make_async_copy(wq_ref, wqF.at[rows_of(dpi, 128)], lsem.at[1]),
           pltpu.make_async_copy(wk_ref, wkF.at[rows_of(dpi, 128)], lsem.at[2])]
    for c in own:
        c.start()
    wh4[rows_of(dpi, 128), lane_block(u)] = wpk[...]
    vgF[rows_of(sp, TOK), :] = vgpack[sp]

    def tables(i, _):
        cols = pl.ds(pl.multiple_of(i * 128, 128), 128)
        c, s = cosT[:, cols], sinT[:, cols]
        tabC[cols, :] = jnp.concatenate([c] * 8, axis=0).T
        tabS[cols, :] = jnp.concatenate([-s, s] * 4, axis=0).T
        return 0
    lax.fori_loop(0, SEQ // 128, tables, 0)
    for c in own:
        c.wait()

    for d in range(2):
        t1_wait(d, 0)
        t1_send(d, 2)
    p1_wait()
    for i in range(2):
        for d in range(2):
            h_send(d, i)
    for k in range(2):
        for d in range(2):
            w_send(d, k)
    for m in range(2):
        mate_own(m)
    for d in range(2):
        t1_wait(d, 1)
        t1_wait(d, 2)
    for d in range(2):
        h_wait(d, 0)
        h_send(d, 2)
    vg_send()
    for d in range(2):
        t2_send(d, 0, 1)
    for d in range(2):
        h_wait(d, 1)
        h_wait(d, 2)

    lane16 = lax.rem(lax.broadcasted_iota(jnp.int32, (TOK, 128), 1), 32) < 16

    def project(i):
        rows = rows_of(spot(u, w + i), TOK)
        r = mm(tokF[rows, :], wh4[...])
        c, s = tabC[rows, :], tabS[rows, :]
        for h in range(4):
            a = r[:, h * 128:(h + 1) * 128]
            other = jnp.where(lane16, pltpu.roll(a, 112, 1), pltpu.roll(a, 16, 1))
            qkS[h, i] = (a * c + other * s).astype(BF16)

    for i in range(4):
        project(i)
        if i:
            qk_send(i - 1)
    for i in range(4):
        rot[rows_of(spot(u, w + i), TOK), :] = qkS[u, i]
    qk_send(3)
    for i in range(1, 4):
        for k in range(2):
            for d in range(2):
                t2_send(d, i, k)
    w_event(0)
    w_event(1)
    vg_wait()

    def turn_vg(i, _):
        r = pl.multiple_of(i * 256, 256)
        vgT[:, pl.ds(r, 256)] = vgF[pl.ds(r, 256), :].astype(F32).T.astype(BF16)
        return 0
    lax.fori_loop(0, SEQ // 256, turn_vg, 0)
    w_event(2)
    t2_event(0)
    qk_wait()

    def turn_qk(i, _):
        r = pl.multiple_of(i * 256, 256)
        rotT[:, pl.ds(r, 256)] = rot[pl.ds(r, 256), :].astype(F32).T.astype(BF16)
        return 0
    lax.fori_loop(0, SEQ // 256, turn_qk, 0)

    batches = ((13, 14, 15), (10, 11, 12), (7, 8, 9), (4, 5, 6), (0, 1, 2, 3))

    def back_one(j):
        @pl.when(sp != j)
        def _():
            send(lambda: bpack.at[j], lambda: bF.at[sp], lambda: bsend.at[j], lambda: brecv.at[sp], lambda: {"sp": j}, lambda: sp != j)

    def back_send(s):
        for j in batches[s]:
            back_one(j)

    plan = {
        (0, 0): [lambda: w_event(3)],
        (0, 1): [lambda: t2_event(1)],
        (1, 0): [lambda: w_event(4), lambda: back_send(0), lambda: t2_event(2)],
        (1, 1): [lambda: w_event(5)],
        (2, 0): [lambda: t2_event(3), lambda: back_send(1)],
        (2, 1): [lambda: w_event(6)],
        (3, 0): [lambda: back_send(2)],
        (4, 0): [lambda: back_send(3)],
    }

    def hook(step, place):
        for (s, p), jobs in plan.items():
            if p == place:
                @pl.when(step == s)
                def _():
                    for job in jobs:
                        job()

    def done(step, b):
        for i in range(BQ // 256):
            cols = pl.ds(pl.multiple_of(b * BQ + i * 256, 256), 256)
            kvT = acc[cols, :].T
            c, s = cosT[:, cols], sinT[:, cols]
            bt = jnp.concatenate([rot_t(dqT[:, cols], c, s, -1.0), rot_t(kvT[0:64], c, s, -1.0)], axis=0)
            backT[:, cols] = bt.astype(BF16)
            xf[cols, :] = bt.T

        first = jnp.where(step == NB - 1, 0, 13 - 3 * step)

        def pack(k, _):
            i = first + k
            r = pl.multiple_of(i * TOK, TOK)
            bpack[i, 0:TOK, :] = xf[pl.ds(r, TOK), :].astype(BF16)
            dv0 = acc[pl.ds(r, HALF), :]
            dv1 = acc[pl.ds(r + HALF, HALF), :]
            bpack[i, TOK:TOK + HALF, :] = jnp.concatenate([dv0[:, 64:], dv1[:, 64:]], axis=1).astype(BF16)
            return 0
        lax.fori_loop(0, jnp.where(step == NB - 1, 4, 3), pack, 0)

    attention(lam_ref[sp], rot, rotT, vgF, vgT, cosT, sinT, dqT, acc, e1, e2, mix, dp, hook, done)
    back_send(4)
    t2_end()

    def dw(i, _):
        cols = pl.ds(pl.multiple_of(i * 256, 256), 256)
        r = mm(backT[...], tokF[:, cols]).astype(BF16)
        dwp[0, i] = r[:, :128]
        dwp[1, i] = r[:, 128:]
        return 0
    lax.fori_loop(0, 8, dw, 0)
    bF[sp] = bpack[sp]
    send(lambda: dwp.at[1 - core], lambda: dwM, lambda: rsend.at[8], lambda: rrecv.at[8], lambda: {"dp": mate})
    mate_end()
    arrive(dwM, rsend.at[8], rrecv.at[8])

    def both(i, _):
        dwP[i] = (dwp[core, i].astype(F32) + dwM[i].astype(F32)).astype(BF16)
        return 0
    lax.fori_loop(0, 8, both, 0)
    for d in (4, 3, 5, 2, 6, 1, 7):
        send(lambda d=d: dwP.at[lax.rem(z + d, 8)], lambda: dwR.at[z], lambda d=d: rsend.at[d], lambda d=d: rrecv.at[d],
             lambda d=d: {"dp": lax.rem(z + d, 8) * 2 + core})
    dwR[z] = dwP[z]
    for d in range(1, 8):
        arrive(dwR.at[lax.rem(z + 8 - d, 8)], rsend.at[d], rrecv.at[d])
    total = dwR[0].astype(F32)
    for i in range(1, 8):
        total += dwR[i].astype(F32)
    total = total.T.astype(BF16)
    dwS[...] = total
    dwG[sp] = total
    for d in (10, 2, 8, 5, 7, 9, 11, 6, 14, 3, 13, 1, 4, 12, 15):
        send(lambda: dwS, lambda: dwG.at[sp], lambda d=d: gsend.at[d], lambda d=d: grecv.at[d], lambda d=d: {"sp": lax.rem(sp + d, 16)})
    for d in range(1, 16):
        j = lax.rem(sp + d, 16)
        arrive(bF.at[j], bsend.at[j], brecv.at[j])

    bq, bk = [], []
    for p in range(8):
        lanes = slice(p * 128, (p + 1) * 128)
        a, b = bF[2 * p], bF[2 * p + 1]
        q, k = join(a[:TOK], b[:TOK])
        bq.append(q)
        bk.append(k)
        top, low = join(a[TOK:], b[TOK:])
        vgrad_ref[0:HALF, lanes] = top
        vgrad_ref[HALF:TOK, lanes] = low
    bq = jnp.concatenate(bq, axis=1)
    bk = jnp.concatenate(bk, axis=1)
    for n in range(8):
        rows = slice(n * 256, (n + 1) * 256)
        tg_ref[:, rows] = (mm(bq, wqF[rows, :], TRANS_B) + mm(bk, wkF[rows, :], TRANS_B)).astype(BF16)

    for d in range(1, 16):
        arrive(dwG.at[lax.rem(sp + 16 - d, 16)], gsend.at[d], grecv.at[d])
    dw_ref[...] = dwG[...]
    for make, when in sends:
        if when is None:
            make().wait_send()
        else:
            pl.when(when())(lambda make=make: make().wait_send())


def settle(factor, tg_ref, vg_ref, dw_ref, tg_out, vg_out, dwq_out, dwk_out):
    tg_out[...] = tg_ref[...]
    vg_out[...] = vg_ref[...]
    for p in range(8):
        lanes = slice(p * 128, (p + 1) * 128)
        q, k = join(dw_ref[2 * p].astype(F32), dw_ref[2 * p + 1].astype(F32))
        dwq_out[:, lanes] = q * factor
        dwk_out[:, lanes] = k * factor


def body(tokens, query_weight, key_weight, values, lambdas, out_grad):
    half = DQK // 2
    freqs = np.exp(np.float32(-math.log(THETA)) * np.arange(half, dtype=np.float32) / np.float32(half))
    angles = freqs[:, None] * np.arange(SEQ, dtype=np.float32)[None, :]
    vm = pl.BlockSpec(memory_space=pltpu.VMEM)
    dma = pltpu.SemaphoreType.DMA
    V = pltpu.VMEM
    return_shapes = (
        jax.ShapeDtypeStruct((TOK, D), BF16),
        jax.ShapeDtypeStruct((TOK, COLS), BF16),
        jax.ShapeDtypeStruct((16, 128, 128), BF16),
    )
    raw = pl.pallas_call(
        kernel,
        out_shape=return_shapes,
        in_specs=[pl.BlockSpec(memory_space=pltpu.SMEM)] + [vm] * 7,
        out_specs=(vm,) * 3,
        scratch_shapes=[
            V((SEQ, D), BF16), V((D, COLS), BF16), V((D, COLS), BF16), V((D, 512), BF16), V((128, 128), BF16),
            V((SEQ, 128), F32), V((SEQ, 128), F32), V((4, 4, TOK, 128), BF16), V((SEQ, 128), F32),
            V((16, TOK, 128), BF16), V((SEQ, 128), BF16),
            V((SEQ, 128), BF16), V((128, SEQ), BF16), V((128, SEQ), BF16), V((64, SEQ), F32), V((SEQ, 128), F32),
            V((SEQ, BQ), F32), V((SEQ, BQ), F32), V((SEQ, BQ), BF16), V((SEQ, BQ), F32),
            V((128, SEQ), BF16), V((16, TOK + HALF, 128), BF16), V((16, TOK + HALF, 128), BF16),
            V((2, 8, 128, 128), BF16), V((8, 128, 128), BF16), V((8, 128, 128), BF16), V((8, 128, 128), BF16), V((128, 128), BF16), V((16, 128, 128), BF16),
            dma((2, 3)), dma((2, 3)), dma((2, 4, 3)), dma((2, 4, 3)), dma((8,)), dma((8,)), dma((8,)), dma((8,)),
            dma((2, 3)), dma((2, 3)), dma((4, 4)), dma((4, 4)),
            dma((2, 7)), dma((2, 7)), dma((16,)), dma((16,)), dma((16,)), dma((16,)),
            dma((16,)), dma((16,)), dma((16,)), dma((16,)), dma((16,)), dma((16,)), dma((3,)),
        ],
        compiler_params=pltpu.CompilerParams(vmem_limit_bytes=62 * 1024 * 1024, collective_id=0, has_side_effects=True),
        name="differential_backward",
    )(lambdas, tokens[0], query_weight, key_weight, values[0], out_grad[0], jnp.asarray(np.cos(angles)), jnp.asarray(np.sin(angles)))
    tg, vg, dq, dk = pl.pallas_call(
        functools.partial(settle, 1.0 / math.sqrt(16 * SEQ)),
        out_shape=(jax.ShapeDtypeStruct((TOK, D), BF16), jax.ShapeDtypeStruct((TOK, COLS), BF16),
                   jax.ShapeDtypeStruct((128, COLS), F32), jax.ShapeDtypeStruct((128, COLS), F32)),
        in_specs=[vm] * 3,
        out_specs=(vm,) * 4,
        name="settle",
    )(*raw)
    return tg[None], vg[None], dq, dk


def solution(mesh):
    in_specs = (
        P("dp", "sp", None),
        P("dp", None),
        P("dp", None),
        P("dp", "sp", None),
        P(),
        P("dp", "sp", None),
    )
    out_specs = (P("dp", "sp", None), P("dp", "sp", None), P("dp", None), P("dp", None))
    return jax.shard_map(body, mesh=mesh, in_specs=in_specs, out_specs=out_specs, check_vma=False)
```

```python
import functools
import math

import jax
import jax.numpy as jnp
import numpy as np
from jax import lax
from jax.experimental import pallas as pl
from jax.experimental.pallas import tpu as pltpu
from jax.sharding import PartitionSpec as P

THETA = 10000.0
DQK = 32
NORM_EPS = 0.1
F32, BF16 = jnp.float32, jnp.bfloat16
SEQ = 2560
BQ = 512
BK = 512
NB = SEQ // BQ


def mm(a, b, dims=(((1,), (0,)), ((), ()))):
    return lax.dot_general(a, b, dims, preferred_element_type=F32)


def rot_t(x, c, s, sign):
    parts = []
    for base in range(0, x.shape[0], 32):
        a, b = x[base:base + 16], x[base + 16:base + 32]
        parts += [a * c - b * (sign * s), b * c + a * (sign * s)]
    return jnp.concatenate(parts, axis=0)


def fold(x, op):
    r = x.reshape(x.shape[0] // 8, 8, x.shape[1])
    return op(r, axis=0)


def attention(lam, rot_ref, rotT_ref, vg_ref, vgT_ref, cosT, sinT, dqT_ref, accT_ref, e1_ref, e2_ref, mix_ref, dp_ref, hook, done):
    inv_root = 1.0 / math.sqrt(32)
    c2 = inv_root * math.log2(math.e)
    accT_ref[...] = jnp.zeros_like(accT_ref)
    zq = jnp.zeros((32, BQ), BF16)

    def block(step, _):
        hook(step, 0)
        b = NB - 1 - step
        qs = pl.multiple_of(b * BQ, BQ)
        qcols = pl.ds(qs, BQ)
        last = b
        q1T = rotT_ref[0:32, qcols]
        q2T = rotT_ref[32:64, qcols]
        rhs1 = jnp.concatenate([zq, zq, q1T, zq], axis=0)
        rhs2 = jnp.concatenate([zq, zq, zq, q2T], axis=0)

        def scores(j):
            ks = pl.multiple_of(j * BK, BK)
            kk = rot_ref[pl.ds(ks, BK), :]
            return ks, mm(kk, rhs1), mm(kk, rhs2)

        def ph1(j, c):
            m1, m2 = c
            ks, s1, s2 = scores(j)
            e1_ref[pl.ds(ks, BK), :] = s1
            e2_ref[pl.ds(ks, BK), :] = s2
            return jnp.maximum(m1, fold(s1, jnp.max)), jnp.maximum(m2, fold(s2, jnp.max))

        neg = jnp.full((8, BQ), -jnp.inf, F32)
        m1, m2 = lax.fori_loop(0, last, ph1, (neg, neg))
        ks, s1, s2 = scores(last)
        mask = (ks + lax.broadcasted_iota(jnp.int32, (BK, BQ), 0)) <= (qs + lax.broadcasted_iota(jnp.int32, (BK, BQ), 1))
        s1 = jnp.where(mask, s1, -jnp.inf)
        s2 = jnp.where(mask, s2, -jnp.inf)
        e1_ref[pl.ds(ks, BK), :] = s1
        e2_ref[pl.ds(ks, BK), :] = s2
        m1 = jnp.max(jnp.maximum(m1, fold(s1, jnp.max)), axis=0, keepdims=True)
        m2 = jnp.max(jnp.maximum(m2, fold(s2, jnp.max)), axis=0, keepdims=True)

        def ph2(j, c):
            l1, l2 = c
            rows = pl.ds(pl.multiple_of(j * BK, BK), BK)
            e1 = jnp.exp2((e1_ref[rows, :] - m1) * c2)
            e2 = jnp.exp2((e2_ref[rows, :] - m2) * c2)
            e1_ref[rows, :] = e1
            e2_ref[rows, :] = e2
            return l1 + fold(e1, jnp.sum), l2 + fold(e2, jnp.sum)

        zero = jnp.zeros((8, BQ), F32)
        l1, l2 = lax.fori_loop(0, last + 1, ph2, (zero, zero))
        r1 = 1.0 / jnp.sum(l1, axis=0, keepdims=True)
        r2 = lam / jnp.sum(l2, axis=0, keepdims=True)

        def ph3(j, o):
            rows = pl.ds(pl.multiple_of(j * BK, BK), BK)
            mix = (e1_ref[rows, :] * r1 - e2_ref[rows, :] * r2).astype(BF16)
            mix_ref[rows, :] = mix
            return o + mm(vgT_ref[0:64, rows], mix)

        o = lax.fori_loop(0, last + 1, ph3, jnp.zeros((64, BQ), F32))
        hook(step, 1)
        g = vgT_ref[64:128, qcols].astype(F32)
        ns = lax.rsqrt(jnp.mean(o * o, axis=0, keepdims=True) + NORM_EPS)
        ob = ns * g - ns * ns * ns * o * jnp.mean(g * o, axis=0, keepdims=True)
        obT = ob.astype(BF16)
        obp = jnp.concatenate([jnp.zeros((64, BQ), F32), ob], axis=0).T.astype(BF16)
        obz = jnp.concatenate([obT, jnp.zeros((64, BQ), BF16)], axis=0)

        def ph4(j, c):
            d1, d2 = c
            rows = pl.ds(pl.multiple_of(j * BK, BK), BK)
            dp = mm(vg_ref[rows, :], obz)
            dp_ref[rows, :] = dp
            return d1 + fold(dp * e1_ref[rows, :], jnp.sum), d2 + fold(dp * e2_ref[rows, :], jnp.sum)

        d1, d2 = lax.fori_loop(0, last + 1, ph4, (zero, zero))
        r2n = -r2
        d1 = jnp.sum(d1, axis=0, keepdims=True) * r1
        d2 = jnp.sum(d2, axis=0, keepdims=True) * (1.0 / jnp.sum(l2, axis=0, keepdims=True))
        f1 = r1 * inv_root
        f2 = r2n * inv_root
        lane = lax.broadcasted_iota(jnp.int32, (BQ, 128), 1)
        qrows = rot_ref[qcols, :]
        zb = jnp.zeros_like(qrows)
        rhs = jnp.concatenate([jnp.where(lane < 32, qrows, zb), jnp.where((lane >= 32) & (lane < 64), qrows, zb), obp], axis=0)

        def ph5(j, c):
            a1, a2 = c
            rows = pl.ds(pl.multiple_of(j * BK, BK), BK)
            dp = dp_ref[rows, :]
            g1 = (e1_ref[rows, :] * f1 * (dp - d1)).astype(BF16)
            g2 = (e2_ref[rows, :] * f2 * (dp - d2)).astype(BF16)
            tb = (((1,), (1,)), ((), ()))
            accT_ref[0:32, rows] += mm(q1T, g1, tb)
            accT_ref[32:64, rows] += mm(q2T, g2, tb)
            accT_ref[64:128, rows] += mm(obT, mix_ref[rows, :], tb)
            return a1 + mm(rotT_ref[64:96, rows], g1), a2 + mm(rotT_ref[96:128, rows], g2)

        za = jnp.zeros((32, BQ), F32)
        a1, a2 = lax.fori_loop(0, last + 1, ph5, (za, za))
        dqT_ref[0:32, qcols] = a1
        dqT_ref[32:64, qcols] = a2
        done(step, b)
        return 0

    lax.fori_loop(0, NB, block, 0)


TOK = 160
HALF = 80
D = 2048
COLS = 1024
TRANS_B = (((1,), (1,)), ((), ()))
MESH = pl.DeviceIdType.MESH


def join(a, b):
    return jnp.concatenate([a[:, :64], b[:, :64]], axis=1), jnp.concatenate([a[:, 64:], b[:, 64:]], axis=1)


def kernel(lam_ref, tok_ref, wq_ref, wk_ref, v_ref, g_ref, cosT, sinT,
           tg_ref, vgrad_ref, dw_ref,
           tokF, wqF, wkF, wh4, wpk, tabC, tabS, qkS, xf, xv, vgpack, vgF, rot, rotT, vgT, dqT, acc, e1, e2, mix, dp,
           backT, bpack, bF, dwp, dwM, dwP, dwR, dwS, dwG,
           t1s, t1r, t2s, t2r, p1s, p1r, m1s, m1r, hs, hr, qs, qr,
           wsend, wrecv, psend, precv, asend, arecv, bsend, brecv, rsend, rrecv, gsend, grecv, lsem):
    sp = lax.axis_index("sp")
    dpi = lax.axis_index("dp")
    core = lax.rem(dpi, 2)
    z = lax.div(dpi, 2)
    mate = z * 2 + 1 - core
    y, x = lax.div(sp, 4), lax.rem(sp, 4)
    u = y * (1 - core) + x * core
    w = x * (1 - core) + y * core

    def spot(uu, ww):
        uu, ww = lax.rem(uu + 4, 4), lax.rem(ww + 4, 4)
        return 4 * (uu * (1 - core) + ww * core) + ww * (1 - core) + uu * core

    barrier = pltpu.get_barrier_semaphore()
    for d in range(1, 16):
        pl.semaphore_signal(barrier, inc=1, device_id={"sp": lax.rem(sp + d, 16)}, device_id_type=MESH)
        pl.semaphore_signal(barrier, inc=1, device_id={"dp": lax.rem(dpi + d, 16)}, device_id_type=MESH)

    pair = pl.ds(pl.multiple_of(lax.div(sp, 2) * 128, 128), 128)
    lo, hi = join(wq_ref[:, pair], wk_ref[:, pair])
    wpk[...] = jnp.where(lax.rem(sp, 2) == 0, lo, hi)

    for p in range(8):
        lanes = slice(p * 128, (p + 1) * 128)
        vgpack[2 * p], vgpack[2 * p + 1] = join(v_ref[:, lanes], g_ref[:, lanes])

    pl.semaphore_wait(barrier, 30)

    sends = []

    def send(src, dst, ss, rs, to, when=None):
        def make():
            return pltpu.make_async_remote_copy(src_ref=src(), dst_ref=dst(), send_sem=ss(), recv_sem=rs(), device_id=to(),
                                                device_id_type=MESH)
        make().start()
        sends.append((make, when))

    def arrive(dst, ss, rs):
        pltpu.make_async_remote_copy(src_ref=dst, dst_ref=dst, send_sem=ss, recv_sem=rs, device_id={"sp": sp},
                                     device_id_type=MESH).wait_recv()

    def rows_of(i, n, at=0, size=None):
        return pl.ds(pl.multiple_of(i * n + at, 16), size or n)

    def t1_go(d):
        return {"sp": spot(u, w + 1 - 2 * d)}

    def t1_part(d, i):
        back = 1 if i < 2 else 2
        half = d if i != 1 else 1 - d
        return rows_of(spot(u, w - back if d == 0 else w + back), TOK, half * HALF, HALF)

    def t1_send(d, i):
        if i < 2:
            half = d if i == 0 else 1 - d
            send(lambda: tok_ref.at[pl.ds(half * HALF, HALF)], lambda: tokF.at[rows_of(sp, TOK, half * HALF, HALF)],
                 lambda: t1s.at[d, i], lambda: t1r.at[d, i], lambda: t1_go(d))
        else:
            send(lambda: tokF.at[t1_part(d, 0)], lambda: tokF.at[t1_part(d, 0)], lambda: t1s.at[d, i], lambda: t1r.at[d, i], lambda: t1_go(d))

    def t1_wait(d, i):
        arrive(tokF.at[t1_part(d, i)], t1s.at[d, i], t1r.at[d, i])

    def t2_go(d):
        return {"sp": spot(u + 1 - 2 * d, w)}

    def t2_rows(d, back, i, half):
        return rows_of(spot(u - back if d == 0 else u + back, w + i), TOK, half * HALF, HALF)

    def t2_send(d, i, k):
        half = d if k != 1 else 1 - d
        part = lambda: tokF.at[t2_rows(d, 1 if k == 2 else 0, i, half)]
        src = (lambda: tok_ref.at[pl.ds(half * HALF, HALF)]) if i == 0 and k < 2 else part
        send(src, part, lambda: t2s.at[d, i, k], lambda: t2r.at[d, i, k], lambda: t2_go(d))

    def t2_wait(d, i, k):
        arrive(tokF.at[t2_rows(d, 2 if k == 2 else 1, i, d if k != 1 else 1 - d)], t2s.at[d, i, k], t2r.at[d, i, k])

    def t2_event(i):
        for d in range(2):
            t2_wait(d, i, 0)
            t2_send(d, i, 2)

    def t2_end():
        for i in range(4):
            for d in range(2):
                t2_wait(d, i, 1)
                t2_wait(d, i, 2)

    def lane_block(i):
        return pl.ds(pl.multiple_of(i * 128, 128), 128)

    def p1_send():
        for d in range(1, 8):
            send(lambda: wpk, lambda: wh4.at[rows_of(dpi, 128), lane_block(u)], lambda d=d: p1s.at[d], lambda d=d: p1r.at[d],
                 lambda d=d: {"dp": lax.rem(z + d, 8) * 2 + core})
        send(lambda: wpk, lambda: wh4.at[rows_of(dpi, 128), lane_block(w)], lambda: m1s.at[0], lambda: m1r.at[0], lambda: {"dp": mate})

    def p1_wait():
        for d in (1, 7, 2, 6, 3, 5, 4):
            part = lambda d=d: wh4.at[rows_of(lax.rem(z + 8 - d, 8) * 2 + core, 128), lane_block(u)]
            to = lambda d=d: wh4.at[rows_of(lax.rem(z + 8 - d, 8) * 2 + core, 128), lane_block(w)]
            arrive(part(), p1s.at[d], p1r.at[d])
            send(part, to, lambda d=d: m1s.at[d], lambda d=d: m1r.at[d], lambda: {"dp": mate})
        for d in range(8):
            arrive(wh4.at[rows_of(lax.rem(z + 8 - d, 8) * 2 + 1 - core, 128), lane_block(u)], m1s.at[d], m1r.at[d])

    def h_part(back, d, half):
        return wh4.at[pl.ds(half * 1024, 1024), lane_block(lax.rem(u + 4 - back if d == 0 else u + back, 4))]

    def h_send(d, i):
        half = d if i != 1 else 1 - d
        part = lambda: h_part(0 if i < 2 else 1, d, half)
        send(part, part, lambda: hs.at[d, i], lambda: hr.at[d, i], lambda: t2_go(d))

    def h_wait(d, i):
        arrive(h_part(1 if i < 2 else 2, d, d if i != 1 else 1 - d), hs.at[d, i], hr.at[d, i])

    wF = (wqF, wkF)
    wown = (wq_ref, wk_ref)

    def w_go(d):
        return {"dp": lax.rem(z + 1 + 6 * d, 8) * 2 + core}

    def w_owner(back, d):
        return lax.rem(z + 8 - back if d == 0 else z + back, 8) * 2 + core

    def w_which(d, k):
        return d if k == 6 else k % 2

    def w_send(d, k):
        m = w_which(d, k)
        send(lambda: wown[m] if k < 2 else wF[m].at[rows_of(w_owner(k // 2, d), 128)], lambda: wF[m].at[rows_of(w_owner(k // 2, d), 128)],
             lambda: wsend.at[d, k], lambda: wrecv.at[d, k], lambda: w_go(d))

    def mate_own(m):
        send(lambda: wown[m], lambda: wF[m].at[rows_of(dpi, 128)], lambda: psend.at[14 + m], lambda: precv.at[14 + m], lambda: {"dp": mate})

    def w_event(k):
        for d in range(2):
            m = w_which(d, k)
            part = lambda m=m, d=d: wF[m].at[rows_of(w_owner(k // 2 + 1, d), 128)]
            arrive(part(), wsend.at[d, k], wrecv.at[d, k])
            if k < 4 or k == 4 + d:
                w_send(d, k + 2 if k < 4 else 6)
            send(part, part, lambda d=d: psend.at[d * 7 + k], lambda d=d: precv.at[d * 7 + k], lambda: {"dp": mate})

    def mate_end():
        for m in range(2):
            arrive(wF[m].at[rows_of(mate, 128)], psend.at[14 + m], precv.at[14 + m])
        for k in range(7):
            for d in range(2):
                arrive(wF[w_which(d, k)].at[rows_of(w_owner(k // 2 + 1, d) + 1 - 2 * core, 128)], psend.at[d * 7 + k], precv.at[d * 7 + k])

    def vg_send():
        for d in range(1, 16):
            send(lambda d=d: vgpack.at[lax.rem(sp + d, 16)], lambda: vgF.at[rows_of(sp, TOK)], lambda d=d: asend.at[d], lambda d=d: arecv.at[d],
                 lambda d=d: {"sp": lax.rem(sp + d, 16)})

    def vg_wait():
        for d in range(1, 16):
            arrive(vgF.at[rows_of(lax.rem(sp + 16 - d, 16), TOK)], asend.at[d], arecv.at[d])

    def qk_send(i):
        for du in (1, 3, 2):
            send(lambda du=du: qkS.at[lax.rem(u + du, 4), i], lambda: rot.at[rows_of(spot(u, w + i), TOK)],
                 lambda du=du: qs.at[du, i], lambda du=du: qr.at[du, i], lambda du=du: {"sp": spot(u + du, w)})

    def qk_wait():
        for du in range(1, 4):
            for i in range(4):
                arrive(rot.at[rows_of(spot(u - du, w + i), TOK)], qs.at[du, i], qr.at[du, i])

    for i in range(2):
        for d in range(2):
            t1_send(d, i)
    p1_send()
    for d in range(2):
        t2_send(d, 0, 0)
    own = [pltpu.make_async_copy(tok_ref, tokF.at[rows_of(sp, TOK)], lsem.at[0]),
           pltpu.make_async_copy(wq_ref, wqF.at[rows_of(dpi, 128)], lsem.at[1]),
           pltpu.make_async_copy(wk_ref, wkF.at[rows_of(dpi, 128)], lsem.at[2])]
    for c in own:
        c.start()
    wh4[rows_of(dpi, 128), lane_block(u)] = wpk[...]
    vgF[rows_of(sp, TOK), :] = vgpack[sp]

    def tables(i, _):
        cols = pl.ds(pl.multiple_of(i * 128, 128), 128)
        c, s = cosT[:, cols], sinT[:, cols]
        tabC[cols, :] = jnp.concatenate([c] * 8, axis=0).T
        tabS[cols, :] = jnp.concatenate([-s, s] * 4, axis=0).T
        return 0
    lax.fori_loop(0, SEQ // 128, tables, 0)
    for c in own:
        c.wait()

    for d in range(2):
        t1_wait(d, 0)
        t1_send(d, 2)
    p1_wait()
    for i in range(2):
        for d in range(2):
            h_send(d, i)
    for k in range(2):
        for d in range(2):
            w_send(d, k)
    for m in range(2):
        mate_own(m)
    for d in range(2):
        t1_wait(d, 1)
        t1_wait(d, 2)
    for d in range(2):
        h_wait(d, 0)
        h_send(d, 2)
    vg_send()
    for d in range(2):
        t2_send(d, 0, 1)
    for d in range(2):
        h_wait(d, 1)
        h_wait(d, 2)

    lane16 = lax.rem(lax.broadcasted_iota(jnp.int32, (TOK, 128), 1), 32) < 16

    def project(i):
        rows = [rows_of(spot(u, w + i + n), TOK) for n in range(2)]
        r = mm(jnp.concatenate([tokF[p, :] for p in rows], axis=0), wh4[...])
        for n in range(2):
            c, s = tabC[rows[n], :], tabS[rows[n], :]
            for h in range(4):
                a = r[n * TOK:(n + 1) * TOK, h * 128:(h + 1) * 128]
                other = jnp.where(lane16, pltpu.roll(a, 112, 1), pltpu.roll(a, 16, 1))
                qkS[h, i + n] = (a * c + other * s).astype(BF16)

    project(0)
    qk_send(0)
    project(2)
    for i in range(1, 4):
        qk_send(i)
    for i in range(4):
        rot[rows_of(spot(u, w + i), TOK), :] = qkS[u, i]
    for i in range(1, 4):
        for k in range(2):
            for d in range(2):
                t2_send(d, i, k)
    w_event(0)
    w_event(1)
    vg_wait()

    def turn_vg(i, _):
        r = pl.multiple_of(i * 256, 256)
        vgT[:, pl.ds(r, 256)] = vgF[pl.ds(r, 256), :].astype(F32).T.astype(BF16)
        return 0
    lax.fori_loop(0, SEQ // 256, turn_vg, 0)
    t2_event(0)
    qk_wait()

    def turn_qk(i, _):
        r = pl.multiple_of(i * 256, 256)
        rotT[:, pl.ds(r, 256)] = rot[pl.ds(r, 256), :].astype(F32).T.astype(BF16)
        return 0
    lax.fori_loop(0, SEQ // 256, turn_qk, 0)

    def back_send():
        for d in (10, 2, 8, 5, 7, 9, 11, 6, 14, 3, 13, 1, 4, 12, 15):
            send(lambda d=d: bpack.at[lax.rem(sp + d, 16)], lambda: bF.at[sp], lambda d=d: bsend.at[d], lambda d=d: brecv.at[d],
                 lambda d=d: {"sp": lax.rem(sp + d, 16)})

    plan = {
        (0, 0): [lambda: w_event(2)],
        (0, 1): [lambda: w_event(3), lambda: t2_event(1)],
        (1, 0): [lambda: w_event(4), lambda: t2_event(2)],
        (1, 1): [lambda: w_event(5), lambda: t2_event(3)],
        (2, 1): [lambda: w_event(6)],
    }

    def hook(step, place):
        for (s, p), jobs in plan.items():
            if p == place:
                @pl.when(step == s)
                def _():
                    for job in jobs:
                        job()

    def done(step, b):
        for i in range(BQ // 256):
            cols = pl.ds(pl.multiple_of(b * BQ + i * 256, 256), 256)
            c, s = cosT[:, cols], sinT[:, cols]
            bt = jnp.concatenate([rot_t(dqT[:, cols], c, s, -1.0), rot_t(acc[0:64, cols], c, s, -1.0)], axis=0)
            backT[:, cols] = bt.astype(BF16)
            xf[cols, :] = bt.T
            xv[cols, :] = acc[64:128, cols].T

        first = jnp.where(step == NB - 1, 0, 13 - 3 * step)

        def pack(k, _):
            i = first + k
            r = pl.multiple_of(i * TOK, TOK)
            bpack[i, 0:TOK, :] = xf[pl.ds(r, TOK), :].astype(BF16)
            bpack[i, TOK:TOK + HALF, :] = jnp.concatenate([xv[pl.ds(r, HALF), :], xv[pl.ds(r + HALF, HALF), :]], axis=1).astype(BF16)
            return 0
        lax.fori_loop(0, jnp.where(step == NB - 1, 4, 3), pack, 0)

    attention(lam_ref[sp], rot, rotT, vgF, vgT, cosT, sinT, dqT, acc, e1, e2, mix, dp, hook, done)
    back_send()
    t2_end()

    def dw(i, _):
        cols = pl.ds(pl.multiple_of(i * 256, 256), 256)
        r = mm(backT[...], tokF[:, cols]).astype(BF16)
        dwp[0, i] = r[:, :128]
        dwp[1, i] = r[:, 128:]
        return 0
    lax.fori_loop(0, 8, dw, 0)
    bF[sp] = bpack[sp]
    send(lambda: dwp.at[1 - core], lambda: dwM, lambda: rsend.at[8], lambda: rrecv.at[8], lambda: {"dp": mate})
    mate_end()
    arrive(dwM, rsend.at[8], rrecv.at[8])

    def both(i, _):
        dwP[i] = (dwp[core, i].astype(F32) + dwM[i].astype(F32)).astype(BF16)
        return 0
    lax.fori_loop(0, 8, both, 0)
    for d in (4, 3, 5, 2, 6, 1, 7):
        send(lambda d=d: dwP.at[lax.rem(z + d, 8)], lambda: dwR.at[z], lambda d=d: rsend.at[d], lambda d=d: rrecv.at[d],
             lambda d=d: {"dp": lax.rem(z + d, 8) * 2 + core})
    dwR[z] = dwP[z]
    for d in range(1, 8):
        arrive(dwR.at[lax.rem(z + 8 - d, 8)], rsend.at[d], rrecv.at[d])
    total = dwR[0].astype(F32)
    for i in range(1, 8):
        total += dwR[i].astype(F32)
    total = total.T.astype(BF16)
    dwS[...] = total
    dwG[sp] = total
    for d in (10, 2, 8, 5, 7, 9, 11, 6, 14, 3, 13, 1, 4, 12, 15):
        send(lambda: dwS, lambda: dwG.at[sp], lambda d=d: gsend.at[d], lambda d=d: grecv.at[d], lambda d=d: {"sp": lax.rem(sp + d, 16)})
    for d in range(1, 16):
        arrive(bF.at[lax.rem(sp + 16 - d, 16)], bsend.at[d], brecv.at[d])

    bq, bk = [], []
    for p in range(8):
        lanes = slice(p * 128, (p + 1) * 128)
        a, b = bF[2 * p], bF[2 * p + 1]
        q, k = join(a[:TOK], b[:TOK])
        bq.append(q)
        bk.append(k)
        top, low = join(a[TOK:], b[TOK:])
        vgrad_ref[0:HALF, lanes] = top
        vgrad_ref[HALF:TOK, lanes] = low
    bq = jnp.concatenate(bq, axis=1)
    bk = jnp.concatenate(bk, axis=1)
    for n in range(8):
        rows = slice(n * 256, (n + 1) * 256)
        tg_ref[:, rows] = (mm(bq, wqF[rows, :], TRANS_B) + mm(bk, wkF[rows, :], TRANS_B)).astype(BF16)

    for d in range(1, 16):
        arrive(dwG.at[lax.rem(sp + 16 - d, 16)], gsend.at[d], grecv.at[d])
    dw_ref[...] = dwG[...]
    for make, when in sends:
        if when is None:
            make().wait_send()
        else:
            pl.when(when())(lambda make=make: make().wait_send())


def settle(factor, tg_ref, vg_ref, dw_ref, tg_out, vg_out, dwq_out, dwk_out):
    tg_out[...] = tg_ref[...]
    vg_out[...] = vg_ref[...]
    for p in range(8):
        lanes = slice(p * 128, (p + 1) * 128)
        q, k = join(dw_ref[2 * p].astype(F32), dw_ref[2 * p + 1].astype(F32))
        dwq_out[:, lanes] = q * factor
        dwk_out[:, lanes] = k * factor


def body(tokens, query_weight, key_weight, values, lambdas, out_grad):
    half = DQK // 2
    freqs = np.exp(np.float32(-math.log(THETA)) * np.arange(half, dtype=np.float32) / np.float32(half))
    angles = freqs[:, None] * np.arange(SEQ, dtype=np.float32)[None, :]
    vm = pl.BlockSpec(memory_space=pltpu.VMEM)
    dma = pltpu.SemaphoreType.DMA
    V = pltpu.VMEM
    return_shapes = (
        jax.ShapeDtypeStruct((TOK, D), BF16),
        jax.ShapeDtypeStruct((TOK, COLS), BF16),
        jax.ShapeDtypeStruct((16, 128, 128), BF16),
    )
    raw = pl.pallas_call(
        kernel,
        out_shape=return_shapes,
        in_specs=[pl.BlockSpec(memory_space=pltpu.SMEM)] + [vm] * 7,
        out_specs=(vm,) * 3,
        scratch_shapes=[
            V((SEQ, D), BF16), V((D, COLS), BF16), V((D, COLS), BF16), V((D, 512), BF16), V((128, 128), BF16),
            V((SEQ, 128), F32), V((SEQ, 128), F32), V((4, 4, TOK, 128), BF16), V((SEQ, 128), F32), V((SEQ, 64), F32),
            V((16, TOK, 128), BF16), V((SEQ, 128), BF16),
            V((SEQ, 128), BF16), V((128, SEQ), BF16), V((128, SEQ), BF16), V((64, SEQ), F32), V((128, SEQ), F32),
            V((SEQ, BQ), F32), V((SEQ, BQ), F32), V((SEQ, BQ), BF16), V((SEQ, BQ), F32),
            V((128, SEQ), BF16), V((16, TOK + HALF, 128), BF16), V((16, TOK + HALF, 128), BF16),
            V((2, 8, 128, 128), BF16), V((8, 128, 128), BF16), V((8, 128, 128), BF16), V((8, 128, 128), BF16), V((128, 128), BF16), V((16, 128, 128), BF16),
            dma((2, 3)), dma((2, 3)), dma((2, 4, 3)), dma((2, 4, 3)), dma((8,)), dma((8,)), dma((8,)), dma((8,)),
            dma((2, 3)), dma((2, 3)), dma((4, 4)), dma((4, 4)),
            dma((2, 7)), dma((2, 7)), dma((16,)), dma((16,)), dma((16,)), dma((16,)),
            dma((16,)), dma((16,)), dma((16,)), dma((16,)), dma((16,)), dma((16,)), dma((3,)),
        ],
        compiler_params=pltpu.CompilerParams(vmem_limit_bytes=62 * 1024 * 1024, collective_id=0, has_side_effects=True),
        name="differential_backward",
    )(lambdas, tokens[0], query_weight, key_weight, values[0], out_grad[0], jnp.asarray(np.cos(angles)), jnp.asarray(np.sin(angles)))
    tg, vg, dq, dk = pl.pallas_call(
        functools.partial(settle, 1.0 / math.sqrt(16 * SEQ)),
        out_shape=(jax.ShapeDtypeStruct((TOK, D), BF16), jax.ShapeDtypeStruct((TOK, COLS), BF16),
                   jax.ShapeDtypeStruct((128, COLS), F32), jax.ShapeDtypeStruct((128, COLS), F32)),
        in_specs=[vm] * 3,
        out_specs=(vm,) * 4,
        name="settle",
    )(*raw)
    return tg[None], vg[None], dq, dk


def solution(mesh):
    in_specs = (
        P("dp", "sp", None),
        P("dp", None),
        P("dp", None),
        P("dp", "sp", None),
        P(),
        P("dp", "sp", None),
    )
    out_specs = (P("dp", "sp", None), P("dp", "sp", None), P("dp", None), P("dp", None))
    return jax.shard_map(body, mesh=mesh, in_specs=in_specs, out_specs=out_specs, check_vma=False)
```

```python
import functools
import math

import jax
import jax.numpy as jnp
import numpy as np
from jax import lax
from jax.experimental import pallas as pl
from jax.experimental.pallas import tpu as pltpu
from jax.sharding import PartitionSpec as P

THETA = 10000.0
DQK = 32
NORM_EPS = 0.1
F32, BF16 = jnp.float32, jnp.bfloat16
SEQ = 2560
BQ = 512
BK = 512
NB = SEQ // BQ


def mm(a, b, dims=(((1,), (0,)), ((), ()))):
    return lax.dot_general(a, b, dims, preferred_element_type=F32)


def rot_t(x, c, s, sign):
    parts = []
    for base in range(0, x.shape[0], 32):
        a, b = x[base:base + 16], x[base + 16:base + 32]
        parts += [a * c - b * (sign * s), b * c + a * (sign * s)]
    return jnp.concatenate(parts, axis=0)


def fold(x, op):
    r = x.reshape(x.shape[0] // 8, 8, x.shape[1])
    return op(r, axis=0)


def attention(lam, rot_ref, rotT_ref, vg_ref, vgT_ref, cosT, sinT, dqT_ref, accT_ref, e1_ref, e2_ref, mix_ref, dp_ref, hook, done):
    inv_root = 1.0 / math.sqrt(32)
    c2 = inv_root * math.log2(math.e)
    accT_ref[...] = jnp.zeros_like(accT_ref)
    zq = jnp.zeros((32, BQ), BF16)

    def block(step, _):
        hook(step, 0)
        b = NB - 1 - step
        qs = pl.multiple_of(b * BQ, BQ)
        qcols = pl.ds(qs, BQ)
        last = b
        q1T = rotT_ref[0:32, qcols]
        q2T = rotT_ref[32:64, qcols]
        rhs1 = jnp.concatenate([zq, zq, q1T, zq], axis=0)
        rhs2 = jnp.concatenate([zq, zq, zq, q2T], axis=0)

        def scores(j):
            ks = pl.multiple_of(j * BK, BK)
            kk = rot_ref[pl.ds(ks, BK), :]
            return ks, mm(kk, rhs1), mm(kk, rhs2)

        def ph1(j, c):
            m1, m2 = c
            ks, s1, s2 = scores(j)
            e1_ref[pl.ds(ks, BK), :] = s1
            e2_ref[pl.ds(ks, BK), :] = s2
            return jnp.maximum(m1, fold(s1, jnp.max)), jnp.maximum(m2, fold(s2, jnp.max))

        neg = jnp.full((8, BQ), -jnp.inf, F32)
        m1, m2 = lax.fori_loop(0, last, ph1, (neg, neg))
        ks, s1, s2 = scores(last)
        mask = (ks + lax.broadcasted_iota(jnp.int32, (BK, BQ), 0)) <= (qs + lax.broadcasted_iota(jnp.int32, (BK, BQ), 1))
        s1 = jnp.where(mask, s1, -jnp.inf)
        s2 = jnp.where(mask, s2, -jnp.inf)
        e1_ref[pl.ds(ks, BK), :] = s1
        e2_ref[pl.ds(ks, BK), :] = s2
        m1 = jnp.max(jnp.maximum(m1, fold(s1, jnp.max)), axis=0, keepdims=True)
        m2 = jnp.max(jnp.maximum(m2, fold(s2, jnp.max)), axis=0, keepdims=True)

        def ph2(j, c):
            l1, l2 = c
            rows = pl.ds(pl.multiple_of(j * BK, BK), BK)
            e1 = jnp.exp2((e1_ref[rows, :] - m1) * c2)
            e2 = jnp.exp2((e2_ref[rows, :] - m2) * c2)
            e1_ref[rows, :] = e1
            e2_ref[rows, :] = e2
            return l1 + fold(e1, jnp.sum), l2 + fold(e2, jnp.sum)

        zero = jnp.zeros((8, BQ), F32)
        l1, l2 = lax.fori_loop(0, last + 1, ph2, (zero, zero))
        r1 = 1.0 / jnp.sum(l1, axis=0, keepdims=True)
        r2 = lam / jnp.sum(l2, axis=0, keepdims=True)

        def ph3(j, o):
            rows = pl.ds(pl.multiple_of(j * BK, BK), BK)
            mix = (e1_ref[rows, :] * r1 - e2_ref[rows, :] * r2).astype(BF16)
            mix_ref[rows, :] = mix
            return o + mm(vgT_ref[0:64, rows], mix)

        o = lax.fori_loop(0, last + 1, ph3, jnp.zeros((64, BQ), F32))
        hook(step, 1)
        g = vgT_ref[64:128, qcols].astype(F32)
        ns = lax.rsqrt(jnp.mean(o * o, axis=0, keepdims=True) + NORM_EPS)
        ob = ns * g - ns * ns * ns * o * jnp.mean(g * o, axis=0, keepdims=True)
        obT = ob.astype(BF16)
        obp = jnp.concatenate([jnp.zeros((64, BQ), F32), ob], axis=0).T.astype(BF16)
        obz = jnp.concatenate([obT, jnp.zeros((64, BQ), BF16)], axis=0)

        def ph4(j, c):
            d1, d2 = c
            rows = pl.ds(pl.multiple_of(j * BK, BK), BK)
            dp = mm(vg_ref[rows, :], obz)
            dp_ref[rows, :] = dp
            return d1 + fold(dp * e1_ref[rows, :], jnp.sum), d2 + fold(dp * e2_ref[rows, :], jnp.sum)

        d1, d2 = lax.fori_loop(0, last + 1, ph4, (zero, zero))
        r2n = -r2
        d1 = jnp.sum(d1, axis=0, keepdims=True) * r1
        d2 = jnp.sum(d2, axis=0, keepdims=True) * (1.0 / jnp.sum(l2, axis=0, keepdims=True))
        f1 = r1 * inv_root
        f2 = r2n * inv_root
        lane = lax.broadcasted_iota(jnp.int32, (BQ, 128), 1)
        qrows = rot_ref[qcols, :]
        zb = jnp.zeros_like(qrows)
        rhs = jnp.concatenate([jnp.where(lane < 32, qrows, zb), jnp.where((lane >= 32) & (lane < 64), qrows, zb), obp], axis=0)

        def ph5(j, c):
            a1, a2 = c
            rows = pl.ds(pl.multiple_of(j * BK, BK), BK)
            dp = dp_ref[rows, :]
            g1 = (e1_ref[rows, :] * f1 * (dp - d1)).astype(BF16)
            g2 = (e2_ref[rows, :] * f2 * (dp - d2)).astype(BF16)
            tb = (((1,), (1,)), ((), ()))
            accT_ref[0:32, rows] += mm(q1T, g1, tb)
            accT_ref[32:64, rows] += mm(q2T, g2, tb)
            accT_ref[64:128, rows] += mm(obT, mix_ref[rows, :], tb)
            return a1 + mm(rotT_ref[64:96, rows], g1), a2 + mm(rotT_ref[96:128, rows], g2)

        za = jnp.zeros((32, BQ), F32)
        a1, a2 = lax.fori_loop(0, last + 1, ph5, (za, za))
        dqT_ref[0:32, qcols] = a1
        dqT_ref[32:64, qcols] = a2
        done(step, b)
        return 0

    lax.fori_loop(0, NB, block, 0)


TOK = 160
HALF = 80
D = 2048
COLS = 1024
TRANS_B = (((1,), (1,)), ((), ()))
MESH = pl.DeviceIdType.MESH


def join(a, b):
    return jnp.concatenate([a[:, :64], b[:, :64]], axis=1), jnp.concatenate([a[:, 64:], b[:, 64:]], axis=1)


def kernel(lam_ref, tok_ref, wq_ref, wk_ref, v_ref, g_ref, cosT, sinT,
           tg_ref, vgrad_ref, dw_ref,
           tokF, wqF, wkF, wh4, wpk, tabC, tabS, qkS, xf, xv, vgpack, vgF, rot, rotT, vgT, dqT, acc, e1, e2, mix, dp,
           backT, bpack, bF, dwp, dwM, dwP, dwR, dwS, dwG,
           t1s, t1r, t2s, t2r, p1s, p1r, m1s, m1r, hs, hr, qs, qr,
           wsend, wrecv, psend, precv, asend, arecv, bsend, brecv, rsend, rrecv, gsend, grecv, g2send, g2recv, lsem):
    sp = lax.axis_index("sp")
    dpi = lax.axis_index("dp")
    core = lax.rem(dpi, 2)
    z = lax.div(dpi, 2)
    mate = z * 2 + 1 - core
    y, x = lax.div(sp, 4), lax.rem(sp, 4)
    u = y * (1 - core) + x * core
    w = x * (1 - core) + y * core

    def spot(uu, ww):
        uu, ww = lax.rem(uu + 4, 4), lax.rem(ww + 4, 4)
        return 4 * (uu * (1 - core) + ww * core) + ww * (1 - core) + uu * core

    barrier = pltpu.get_barrier_semaphore()
    for d in range(1, 16):
        pl.semaphore_signal(barrier, inc=1, device_id={"sp": lax.rem(sp + d, 16)}, device_id_type=MESH)
        pl.semaphore_signal(barrier, inc=1, device_id={"dp": lax.rem(dpi + d, 16)}, device_id_type=MESH)

    pair = pl.ds(pl.multiple_of(lax.div(sp, 2) * 128, 128), 128)
    lo, hi = join(wq_ref[:, pair], wk_ref[:, pair])
    wpk[...] = jnp.where(lax.rem(sp, 2) == 0, lo, hi)

    for p in range(8):
        lanes = slice(p * 128, (p + 1) * 128)
        vgpack[2 * p], vgpack[2 * p + 1] = join(v_ref[:, lanes], g_ref[:, lanes])

    pl.semaphore_wait(barrier, 30)

    sends = []

    def send(src, dst, ss, rs, to, when=None):
        def make():
            return pltpu.make_async_remote_copy(src_ref=src(), dst_ref=dst(), send_sem=ss(), recv_sem=rs(), device_id=to(),
                                                device_id_type=MESH)
        make().start()
        sends.append((make, when))

    def arrive(dst, ss, rs):
        pltpu.make_async_remote_copy(src_ref=dst, dst_ref=dst, send_sem=ss, recv_sem=rs, device_id={"sp": sp},
                                     device_id_type=MESH).wait_recv()

    def rows_of(i, n, at=0, size=None):
        return pl.ds(pl.multiple_of(i * n + at, 16), size or n)

    def t1_go(d):
        return {"sp": spot(u, w + 1 - 2 * d)}

    def t1_part(d, i):
        back = 1 if i < 2 else 2
        half = d if i != 1 else 1 - d
        return rows_of(spot(u, w - back if d == 0 else w + back), TOK, half * HALF, HALF)

    def t1_send(d, i):
        if i < 2:
            half = d if i == 0 else 1 - d
            send(lambda: tok_ref.at[pl.ds(half * HALF, HALF)], lambda: tokF.at[rows_of(sp, TOK, half * HALF, HALF)],
                 lambda: t1s.at[d, i], lambda: t1r.at[d, i], lambda: t1_go(d))
        else:
            send(lambda: tokF.at[t1_part(d, 0)], lambda: tokF.at[t1_part(d, 0)], lambda: t1s.at[d, i], lambda: t1r.at[d, i], lambda: t1_go(d))

    def t1_wait(d, i):
        arrive(tokF.at[t1_part(d, i)], t1s.at[d, i], t1r.at[d, i])

    def t2_go(d):
        return {"sp": spot(u + 1 - 2 * d, w)}

    def t2_rows(d, back, i, half):
        return rows_of(spot(u - back if d == 0 else u + back, w + i), TOK, half * HALF, HALF)

    def t2_send(d, i, k):
        half = d if k != 1 else 1 - d
        part = lambda: tokF.at[t2_rows(d, 1 if k == 2 else 0, i, half)]
        src = (lambda: tok_ref.at[pl.ds(half * HALF, HALF)]) if i == 0 and k < 2 else part
        send(src, part, lambda: t2s.at[d, i, k], lambda: t2r.at[d, i, k], lambda: t2_go(d))

    def t2_wait(d, i, k):
        arrive(tokF.at[t2_rows(d, 2 if k == 2 else 1, i, d if k != 1 else 1 - d)], t2s.at[d, i, k], t2r.at[d, i, k])

    def t2_event(i):
        for d in range(2):
            t2_wait(d, i, 0)
            t2_send(d, i, 2)

    def t2_end():
        for i in range(4):
            for d in range(2):
                t2_wait(d, i, 1)
                t2_wait(d, i, 2)

    def lane_block(i):
        return pl.ds(pl.multiple_of(i * 128, 128), 128)

    def p1_send():
        for d in range(1, 8):
            send(lambda: wpk, lambda: wh4.at[rows_of(dpi, 128), lane_block(u)], lambda d=d: p1s.at[d], lambda d=d: p1r.at[d],
                 lambda d=d: {"dp": lax.rem(z + d, 8) * 2 + core})
        send(lambda: wpk, lambda: wh4.at[rows_of(dpi, 128), lane_block(w)], lambda: m1s.at[0], lambda: m1r.at[0], lambda: {"dp": mate})

    def p1_wait():
        for d in (1, 7, 2, 6, 3, 5, 4):
            part = lambda d=d: wh4.at[rows_of(lax.rem(z + 8 - d, 8) * 2 + core, 128), lane_block(u)]
            to = lambda d=d: wh4.at[rows_of(lax.rem(z + 8 - d, 8) * 2 + core, 128), lane_block(w)]
            arrive(part(), p1s.at[d], p1r.at[d])
            send(part, to, lambda d=d: m1s.at[d], lambda d=d: m1r.at[d], lambda: {"dp": mate})
        for d in range(8):
            arrive(wh4.at[rows_of(lax.rem(z + 8 - d, 8) * 2 + 1 - core, 128), lane_block(u)], m1s.at[d], m1r.at[d])

    def h_part(back, d, half):
        return wh4.at[pl.ds(half * 1024, 1024), lane_block(lax.rem(u + 4 - back if d == 0 else u + back, 4))]

    def h_send(d, i):
        half = d if i != 1 else 1 - d
        part = lambda: h_part(0 if i < 2 else 1, d, half)
        send(part, part, lambda: hs.at[d, i], lambda: hr.at[d, i], lambda: t2_go(d))

    def h_wait(d, i):
        arrive(h_part(1 if i < 2 else 2, d, d if i != 1 else 1 - d), hs.at[d, i], hr.at[d, i])

    wF = (wqF, wkF)
    wown = (wq_ref, wk_ref)

    def w_go(d):
        return {"dp": lax.rem(z + 1 + 6 * d, 8) * 2 + core}

    def w_owner(back, d):
        return lax.rem(z + 8 - back if d == 0 else z + back, 8) * 2 + core

    def w_which(d, k):
        return d if k == 6 else k % 2

    def w_send(d, k):
        m = w_which(d, k)
        send(lambda: wown[m] if k < 2 else wF[m].at[rows_of(w_owner(k // 2, d), 128)], lambda: wF[m].at[rows_of(w_owner(k // 2, d), 128)],
             lambda: wsend.at[d, k], lambda: wrecv.at[d, k], lambda: w_go(d))

    def mate_own(m):
        send(lambda: wown[m], lambda: wF[m].at[rows_of(dpi, 128)], lambda: psend.at[14 + m], lambda: precv.at[14 + m], lambda: {"dp": mate})

    def w_event(k):
        for d in range(2):
            m = w_which(d, k)
            part = lambda m=m, d=d: wF[m].at[rows_of(w_owner(k // 2 + 1, d), 128)]
            arrive(part(), wsend.at[d, k], wrecv.at[d, k])
            if k < 4 or k == 4 + d:
                w_send(d, k + 2 if k < 4 else 6)
            send(part, part, lambda d=d: psend.at[d * 7 + k], lambda d=d: precv.at[d * 7 + k], lambda: {"dp": mate})

    def mate_end():
        for m in range(2):
            arrive(wF[m].at[rows_of(mate, 128)], psend.at[14 + m], precv.at[14 + m])
        for k in range(7):
            for d in range(2):
                arrive(wF[w_which(d, k)].at[rows_of(w_owner(k // 2 + 1, d) + 1 - 2 * core, 128)], psend.at[d * 7 + k], precv.at[d * 7 + k])

    def vg_send():
        for d in range(1, 16):
            send(lambda d=d: vgpack.at[lax.rem(sp + d, 16)], lambda: vgF.at[rows_of(sp, TOK)], lambda d=d: asend.at[d], lambda d=d: arecv.at[d],
                 lambda d=d: {"sp": lax.rem(sp + d, 16)})

    def vg_wait():
        for d in range(1, 16):
            arrive(vgF.at[rows_of(lax.rem(sp + 16 - d, 16), TOK)], asend.at[d], arecv.at[d])

    def qk_send(i):
        for du in (1, 3, 2):
            send(lambda du=du: qkS.at[lax.rem(u + du, 4), i], lambda: rot.at[rows_of(spot(u, w + i), TOK)],
                 lambda du=du: qs.at[du, i], lambda du=du: qr.at[du, i], lambda du=du: {"sp": spot(u + du, w)})

    def qk_wait():
        for du in range(1, 4):
            for i in range(4):
                arrive(rot.at[rows_of(spot(u - du, w + i), TOK)], qs.at[du, i], qr.at[du, i])

    for i in range(2):
        for d in range(2):
            t1_send(d, i)
    p1_send()
    for d in range(2):
        t2_send(d, 0, 0)
    own = [pltpu.make_async_copy(tok_ref, tokF.at[rows_of(sp, TOK)], lsem.at[0]),
           pltpu.make_async_copy(wq_ref, wqF.at[rows_of(dpi, 128)], lsem.at[1]),
           pltpu.make_async_copy(wk_ref, wkF.at[rows_of(dpi, 128)], lsem.at[2])]
    for c in own:
        c.start()
    wh4[rows_of(dpi, 128), lane_block(u)] = wpk[...]
    vgF[rows_of(sp, TOK), :] = vgpack[sp]

    def tables(i, _):
        cols = pl.ds(pl.multiple_of(i * 128, 128), 128)
        c, s = cosT[:, cols], sinT[:, cols]
        tabC[cols, :] = jnp.concatenate([c] * 8, axis=0).T
        tabS[cols, :] = jnp.concatenate([-s, s] * 4, axis=0).T
        return 0
    lax.fori_loop(0, SEQ // 128, tables, 0)
    for c in own:
        c.wait()

    for d in range(2):
        t1_wait(d, 0)
        t1_send(d, 2)
    p1_wait()
    for i in range(2):
        for d in range(2):
            h_send(d, i)
    for d in range(2):
        t1_wait(d, 1)
        t1_wait(d, 2)
    for d in range(2):
        h_wait(d, 0)
        h_send(d, 2)
    vg_send()
    for d in range(2):
        t2_send(d, 0, 1)
    for k in range(2):
        for d in range(2):
            w_send(d, k)
    for m in range(2):
        mate_own(m)
    for d in range(2):
        h_wait(d, 1)
        h_wait(d, 2)

    lane16 = lax.rem(lax.broadcasted_iota(jnp.int32, (TOK, 128), 1), 32) < 16

    def project(i):
        rows = [rows_of(spot(u, w + i + n), TOK) for n in range(2)]
        r = mm(jnp.concatenate([tokF[p, :] for p in rows], axis=0), wh4[...])
        for n in range(2):
            c, s = tabC[rows[n], :], tabS[rows[n], :]
            for h in range(4):
                a = r[n * TOK:(n + 1) * TOK, h * 128:(h + 1) * 128]
                other = jnp.where(lane16, pltpu.roll(a, 112, 1), pltpu.roll(a, 16, 1))
                qkS[h, i + n] = (a * c + other * s).astype(BF16)

    project(0)
    qk_send(0)
    project(2)
    for i in range(1, 4):
        qk_send(i)
    for i in range(4):
        rot[rows_of(spot(u, w + i), TOK), :] = qkS[u, i]
    for i in range(1, 4):
        for k in range(2):
            for d in range(2):
                t2_send(d, i, k)
    w_event(0)
    vg_wait()

    def turn_vg(i, _):
        r = pl.multiple_of(i * 256, 256)
        vgT[:, pl.ds(r, 256)] = vgF[pl.ds(r, 256), :].astype(F32).T.astype(BF16)
        return 0
    lax.fori_loop(0, SEQ // 256, turn_vg, 0)
    qk_wait()

    def turn_qk(i, _):
        r = pl.multiple_of(i * 256, 256)
        rotT[:, pl.ds(r, 256)] = rot[pl.ds(r, 256), :].astype(F32).T.astype(BF16)
        return 0
    lax.fori_loop(0, SEQ // 256, turn_qk, 0)

    def back_send():
        for d in (10, 2, 8, 5, 7, 9, 11, 6, 14, 3, 13, 1, 4, 12, 15):
            send(lambda d=d: bpack.at[lax.rem(sp + d, 16)], lambda: bF.at[sp], lambda d=d: bsend.at[d], lambda d=d: brecv.at[d],
                 lambda d=d: {"sp": lax.rem(sp + d, 16)})

    plan = {
        (0, 0): [lambda: w_event(1)],
        (0, 1): [lambda: w_event(2), lambda: t2_event(0)],
        (1, 0): [lambda: w_event(3), lambda: t2_event(1)],
        (1, 1): [lambda: w_event(4), lambda: t2_event(2)],
        (2, 0): [lambda: w_event(5), lambda: t2_event(3)],
        (3, 0): [lambda: w_event(6)],
    }

    def hook(step, place):
        for (s, p), jobs in plan.items():
            if p == place:
                @pl.when(step == s)
                def _():
                    for job in jobs:
                        job()

    def done(step, b):
        for i in range(BQ // 256):
            cols = pl.ds(pl.multiple_of(b * BQ + i * 256, 256), 256)
            c, s = cosT[:, cols], sinT[:, cols]
            bt = jnp.concatenate([rot_t(dqT[:, cols], c, s, -1.0), rot_t(acc[0:64, cols], c, s, -1.0)], axis=0)
            backT[:, cols] = bt.astype(BF16)
            xf[cols, :] = bt.T
            xv[cols, :] = acc[64:128, cols].T

        first = jnp.where(step == NB - 1, 0, 13 - 3 * step)

        def pack(k, _):
            i = first + k
            r = pl.multiple_of(i * TOK, TOK)
            bpack[i, 0:TOK, :] = xf[pl.ds(r, TOK), :].astype(BF16)
            bpack[i, TOK:TOK + HALF, :] = jnp.concatenate([xv[pl.ds(r, HALF), :], xv[pl.ds(r + HALF, HALF), :]], axis=1).astype(BF16)
            return 0
        lax.fori_loop(0, jnp.where(step == NB - 1, 4, 3), pack, 0)

    attention(lam_ref[sp], rot, rotT, vgF, vgT, cosT, sinT, dqT, acc, e1, e2, mix, dp, hook, done)
    back_send()
    t2_end()

    far = (4, 3, 5, 2, 6, 1, 7, 0)

    def chip(i):
        return lax.rem(z + far[i], 8)

    def piece(i):
        r = mm(backT[...], tokF[:, pl.ds(pl.multiple_of(chip(i) * 256, 256), 256)]).astype(BF16)
        dwp[0, chip(i)] = r[:, :128]
        dwp[1, chip(i)] = r[:, 128:]

    def piece_mate(i):
        send(lambda: dwp.at[1 - core, chip(i)], lambda: dwM.at[chip(i)], lambda: rsend.at[8 + i], lambda: rrecv.at[8 + i], lambda: {"dp": mate})

    def piece_add(i):
        arrive(dwM.at[chip(i)], rsend.at[8 + i], rrecv.at[8 + i])
        both = (dwp[core, chip(i)].astype(F32) + dwM[chip(i)].astype(F32)).astype(BF16)
        dwP[chip(i)] = both
        if far[i] == 0:
            dwR[z] = both

    def piece_go(i):
        if far[i]:
            send(lambda: dwP.at[chip(i)], lambda: dwR.at[z], lambda: rsend.at[far[i]], lambda: rrecv.at[far[i]], lambda: {"dp": chip(i) * 2 + core})

    for t in range(15):
        for job, late in ((piece, 0), (piece_mate, 1), (piece_add, 5), (piece_go, 6)):
            if 0 <= t - late < 8:
                job(t - late)
    bF[sp] = bpack[sp]
    mate_end()
    for d in range(1, 8):
        arrive(dwR.at[lax.rem(z + 8 - d, 8)], rsend.at[d], rrecv.at[d])
    total = dwR[0].astype(F32)
    for i in range(1, 8):
        total += dwR[i].astype(F32)
    total = total.T.astype(BF16)
    dwS[...] = total
    dwG[sp] = total

    def row_send(dw):
        send(lambda: dwS, lambda: dwG.at[sp], lambda: gsend.at[dw], lambda: grecv.at[dw], lambda: {"sp": spot(u, w + dw)})

    def column_send(i):
        for du in (2, 1, 3):
            send(lambda: dwS if i == 0 else dwG.at[spot(u, w - i)], lambda: dwG.at[spot(u, w - i)], lambda du=du: g2send.at[du, i],
                 lambda du=du: g2recv.at[du, i], lambda du=du: {"sp": spot(u + du, w)})

    for dw in (2, 1, 3):
        row_send(dw)
    column_send(0)
    for d in range(1, 16):
        arrive(bF.at[lax.rem(sp + 16 - d, 16)], bsend.at[d], brecv.at[d])

    bq, bk = [], []
    for p in range(8):
        lanes = slice(p * 128, (p + 1) * 128)
        a, b = bF[2 * p], bF[2 * p + 1]
        q, k = join(a[:TOK], b[:TOK])
        bq.append(q)
        bk.append(k)
        top, low = join(a[TOK:], b[TOK:])
        vgrad_ref[0:HALF, lanes] = top
        vgrad_ref[HALF:TOK, lanes] = low
    bq = jnp.concatenate(bq, axis=1)
    bk = jnp.concatenate(bk, axis=1)
    for i in (1, 3, 2):
        arrive(dwG.at[spot(u, w - i)], gsend.at[i], grecv.at[i])
        column_send(i)
    for n in range(8):
        rows = slice(n * 256, (n + 1) * 256)
        tg_ref[:, rows] = (mm(bq, wqF[rows, :], TRANS_B) + mm(bk, wkF[rows, :], TRANS_B)).astype(BF16)

    for i in range(4):
        for du in range(1, 4):
            arrive(dwG.at[spot(u - du, w - i)], g2send.at[du, i], g2recv.at[du, i])
    dw_ref[...] = dwG[...]
    for make, when in sends:
        if when is None:
            make().wait_send()
        else:
            pl.when(when())(lambda make=make: make().wait_send())


def settle(factor, tg_ref, vg_ref, dw_ref, tg_out, vg_out, dwq_out, dwk_out):
    tg_out[...] = tg_ref[...]
    vg_out[...] = vg_ref[...]
    for p in range(8):
        lanes = slice(p * 128, (p + 1) * 128)
        q, k = join(dw_ref[2 * p].astype(F32), dw_ref[2 * p + 1].astype(F32))
        dwq_out[:, lanes] = q * factor
        dwk_out[:, lanes] = k * factor


def body(tokens, query_weight, key_weight, values, lambdas, out_grad):
    half = DQK // 2
    freqs = np.exp(np.float32(-math.log(THETA)) * np.arange(half, dtype=np.float32) / np.float32(half))
    angles = freqs[:, None] * np.arange(SEQ, dtype=np.float32)[None, :]
    vm = pl.BlockSpec(memory_space=pltpu.VMEM)
    dma = pltpu.SemaphoreType.DMA
    V = pltpu.VMEM
    return_shapes = (
        jax.ShapeDtypeStruct((TOK, D), BF16),
        jax.ShapeDtypeStruct((TOK, COLS), BF16),
        jax.ShapeDtypeStruct((16, 128, 128), BF16),
    )
    raw = pl.pallas_call(
        kernel,
        out_shape=return_shapes,
        in_specs=[pl.BlockSpec(memory_space=pltpu.SMEM)] + [vm] * 7,
        out_specs=(vm,) * 3,
        scratch_shapes=[
            V((SEQ, D), BF16), V((D, COLS), BF16), V((D, COLS), BF16), V((D, 512), BF16), V((128, 128), BF16),
            V((SEQ, 128), F32), V((SEQ, 128), F32), V((4, 4, TOK, 128), BF16), V((SEQ, 128), F32), V((SEQ, 64), F32),
            V((16, TOK, 128), BF16), V((SEQ, 128), BF16),
            V((SEQ, 128), BF16), V((128, SEQ), BF16), V((128, SEQ), BF16), V((64, SEQ), F32), V((128, SEQ), F32),
            V((SEQ, BQ), F32), V((SEQ, BQ), F32), V((SEQ, BQ), BF16), V((SEQ, BQ), F32),
            V((128, SEQ), BF16), V((16, TOK + HALF, 128), BF16), V((16, TOK + HALF, 128), BF16),
            V((2, 8, 128, 128), BF16), V((8, 128, 128), BF16), V((8, 128, 128), BF16), V((8, 128, 128), BF16), V((128, 128), BF16), V((16, 128, 128), BF16),
            dma((2, 3)), dma((2, 3)), dma((2, 4, 3)), dma((2, 4, 3)), dma((8,)), dma((8,)), dma((8,)), dma((8,)),
            dma((2, 3)), dma((2, 3)), dma((4, 4)), dma((4, 4)),
            dma((2, 7)), dma((2, 7)), dma((16,)), dma((16,)), dma((16,)), dma((16,)),
            dma((16,)), dma((16,)), dma((16,)), dma((16,)), dma((4,)), dma((4,)), dma((4, 4)), dma((4, 4)), dma((3,)),
        ],
        compiler_params=pltpu.CompilerParams(vmem_limit_bytes=62 * 1024 * 1024, collective_id=0, has_side_effects=True),
        name="differential_backward",
    )(lambdas, tokens[0], query_weight, key_weight, values[0], out_grad[0], jnp.asarray(np.cos(angles)), jnp.asarray(np.sin(angles)))
    tg, vg, dq, dk = pl.pallas_call(
        functools.partial(settle, 1.0 / math.sqrt(16 * SEQ)),
        out_shape=(jax.ShapeDtypeStruct((TOK, D), BF16), jax.ShapeDtypeStruct((TOK, COLS), BF16),
                   jax.ShapeDtypeStruct((128, COLS), F32), jax.ShapeDtypeStruct((128, COLS), F32)),
        in_specs=[vm] * 3,
        out_specs=(vm,) * 4,
        name="settle",
    )(*raw)
    return tg[None], vg[None], dq, dk


def solution(mesh):
    in_specs = (
        P("dp", "sp", None),
        P("dp", None),
        P("dp", None),
        P("dp", "sp", None),
        P(),
        P("dp", "sp", None),
    )
    out_specs = (P("dp", "sp", None), P("dp", "sp", None), P("dp", None), P("dp", None))
    return jax.shard_map(body, mesh=mesh, in_specs=in_specs, out_specs=out_specs, check_vma=False)
```

```python
import functools
import math

import jax
import jax.numpy as jnp
import numpy as np
from jax import lax
from jax.experimental import pallas as pl
from jax.experimental.pallas import tpu as pltpu
from jax.sharding import PartitionSpec as P

THETA = 10000.0
DQK = 32
NORM_EPS = 0.1
F32, BF16 = jnp.float32, jnp.bfloat16
SEQ = 2560
BQ = 512
BK = 512
NB = SEQ // BQ


def mm(a, b, dims=(((1,), (0,)), ((), ()))):
    return lax.dot_general(a, b, dims, preferred_element_type=F32)


def rot_t(x, c, s, sign):
    parts = []
    for base in range(0, x.shape[0], 32):
        a, b = x[base:base + 16], x[base + 16:base + 32]
        parts += [a * c - b * (sign * s), b * c + a * (sign * s)]
    return jnp.concatenate(parts, axis=0)


def fold(x, op):
    r = x.reshape(x.shape[0] // 8, 8, x.shape[1])
    return op(r, axis=0)


def attention(lam, rot_ref, rotT_ref, vg_ref, vgT_ref, cosT, sinT, dqT_ref, accT_ref, e1_ref, e2_ref, mix_ref, dp_ref, hook, done):
    inv_root = 1.0 / math.sqrt(32)
    c2 = inv_root * math.log2(math.e)
    accT_ref[...] = jnp.zeros_like(accT_ref)
    zq = jnp.zeros((32, BQ), BF16)

    def block(step, _):
        hook(step, 0)
        b = NB - 1 - step
        qs = pl.multiple_of(b * BQ, BQ)
        qcols = pl.ds(qs, BQ)
        last = b
        q1T = rotT_ref[0:32, qcols]
        q2T = rotT_ref[32:64, qcols]
        rhs1 = jnp.concatenate([zq, zq, q1T, zq], axis=0)
        rhs2 = jnp.concatenate([zq, zq, zq, q2T], axis=0)

        def scores(j):
            ks = pl.multiple_of(j * BK, BK)
            kk = rot_ref[pl.ds(ks, BK), :]
            return ks, mm(kk, rhs1), mm(kk, rhs2)

        def ph1(j, c):
            m1, m2 = c
            ks, s1, s2 = scores(j)
            e1_ref[pl.ds(ks, BK), :] = s1
            e2_ref[pl.ds(ks, BK), :] = s2
            return jnp.maximum(m1, fold(s1, jnp.max)), jnp.maximum(m2, fold(s2, jnp.max))

        neg = jnp.full((8, BQ), -jnp.inf, F32)
        m1, m2 = lax.fori_loop(0, last, ph1, (neg, neg))
        ks, s1, s2 = scores(last)
        mask = (ks + lax.broadcasted_iota(jnp.int32, (BK, BQ), 0)) <= (qs + lax.broadcasted_iota(jnp.int32, (BK, BQ), 1))
        s1 = jnp.where(mask, s1, -jnp.inf)
        s2 = jnp.where(mask, s2, -jnp.inf)
        e1_ref[pl.ds(ks, BK), :] = s1
        e2_ref[pl.ds(ks, BK), :] = s2
        m1 = jnp.max(jnp.maximum(m1, fold(s1, jnp.max)), axis=0, keepdims=True)
        m2 = jnp.max(jnp.maximum(m2, fold(s2, jnp.max)), axis=0, keepdims=True)

        def ph2(j, c):
            l1, l2 = c
            rows = pl.ds(pl.multiple_of(j * BK, BK), BK)
            e1 = jnp.exp2((e1_ref[rows, :] - m1) * c2)
            e2 = jnp.exp2((e2_ref[rows, :] - m2) * c2)
            e1_ref[rows, :] = e1
            e2_ref[rows, :] = e2
            return l1 + fold(e1, jnp.sum), l2 + fold(e2, jnp.sum)

        zero = jnp.zeros((8, BQ), F32)
        l1, l2 = lax.fori_loop(0, last + 1, ph2, (zero, zero))
        r1 = 1.0 / jnp.sum(l1, axis=0, keepdims=True)
        r2 = lam / jnp.sum(l2, axis=0, keepdims=True)

        def ph3(j, o):
            rows = pl.ds(pl.multiple_of(j * BK, BK), BK)
            mix = (e1_ref[rows, :] * r1 - e2_ref[rows, :] * r2).astype(BF16)
            mix_ref[rows, :] = mix
            return o + mm(vgT_ref[0:64, rows], mix)

        o = lax.fori_loop(0, last + 1, ph3, jnp.zeros((64, BQ), F32))
        hook(step, 1)
        g = vgT_ref[64:128, qcols].astype(F32)
        ns = lax.rsqrt(jnp.mean(o * o, axis=0, keepdims=True) + NORM_EPS)
        ob = ns * g - ns * ns * ns * o * jnp.mean(g * o, axis=0, keepdims=True)
        obT = ob.astype(BF16)
        obp = jnp.concatenate([jnp.zeros((64, BQ), F32), ob], axis=0).T.astype(BF16)
        obz = jnp.concatenate([obT, jnp.zeros((64, BQ), BF16)], axis=0)

        def ph4(j, c):
            d1, d2 = c
            rows = pl.ds(pl.multiple_of(j * BK, BK), BK)
            dp = mm(vg_ref[rows, :], obz)
            dp_ref[rows, :] = dp
            return d1 + fold(dp * e1_ref[rows, :], jnp.sum), d2 + fold(dp * e2_ref[rows, :], jnp.sum)

        d1, d2 = lax.fori_loop(0, last + 1, ph4, (zero, zero))
        r2n = -r2
        d1 = jnp.sum(d1, axis=0, keepdims=True) * r1
        d2 = jnp.sum(d2, axis=0, keepdims=True) * (1.0 / jnp.sum(l2, axis=0, keepdims=True))
        f1 = r1 * inv_root
        f2 = r2n * inv_root
        lane = lax.broadcasted_iota(jnp.int32, (BQ, 128), 1)
        qrows = rot_ref[qcols, :]
        zb = jnp.zeros_like(qrows)
        rhs = jnp.concatenate([jnp.where(lane < 32, qrows, zb), jnp.where((lane >= 32) & (lane < 64), qrows, zb), obp], axis=0)

        def ph5(j, c):
            a1, a2 = c
            rows = pl.ds(pl.multiple_of(j * BK, BK), BK)
            dp = dp_ref[rows, :]
            g1 = (e1_ref[rows, :] * f1 * (dp - d1)).astype(BF16)
            g2 = (e2_ref[rows, :] * f2 * (dp - d2)).astype(BF16)
            tb = (((1,), (1,)), ((), ()))
            accT_ref[0:32, rows] += mm(q1T, g1, tb)
            accT_ref[32:64, rows] += mm(q2T, g2, tb)
            accT_ref[64:128, rows] += mm(obT, mix_ref[rows, :], tb)
            return a1 + mm(rotT_ref[64:96, rows], g1), a2 + mm(rotT_ref[96:128, rows], g2)

        za = jnp.zeros((32, BQ), F32)
        a1, a2 = lax.fori_loop(0, last + 1, ph5, (za, za))
        dqT_ref[0:32, qcols] = a1
        dqT_ref[32:64, qcols] = a2
        done(step, b)
        return 0

    lax.fori_loop(0, NB, block, 0)


TOK = 160
HALF = 80
D = 2048
COLS = 1024
TRANS_B = (((1,), (1,)), ((), ()))
MESH = pl.DeviceIdType.MESH


def join(a, b):
    return jnp.concatenate([a[:, :64], b[:, :64]], axis=1), jnp.concatenate([a[:, 64:], b[:, 64:]], axis=1)


def kernel(lam_ref, tok_ref, wq_ref, wk_ref, v_ref, g_ref, cosT, sinT,
           tg_ref, vgrad_ref, dw_ref,
           tokF, wqF, wkF, wh4, wpk, tabC, tabS, qkS, xf, xv, vgpack, vgF, rot, rotT, vgT, dqT, acc, e1, e2, mix, dp,
           backT, bpack, bF, dwp, dwM, dwP, dwR, dwS, dwG,
           t1s, t1r, t2s, t2r, p1s, p1r, m1s, m1r, hs, hr, qs, qr,
           wsend, wrecv, psend, precv, asend, arecv, bsend, brecv, rsend, rrecv, gsend, grecv, g2send, g2recv, lsem):
    sp = lax.axis_index("sp")
    dpi = lax.axis_index("dp")
    core = lax.rem(dpi, 2)
    z = lax.div(dpi, 2)
    mate = z * 2 + 1 - core
    y, x = lax.div(sp, 4), lax.rem(sp, 4)
    u = y * (1 - core) + x * core
    w = x * (1 - core) + y * core

    def spot(uu, ww):
        uu, ww = lax.rem(uu + 4, 4), lax.rem(ww + 4, 4)
        return 4 * (uu * (1 - core) + ww * core) + ww * (1 - core) + uu * core

    barrier = pltpu.get_barrier_semaphore()
    for d in range(1, 16):
        pl.semaphore_signal(barrier, inc=1, device_id={"sp": lax.rem(sp + d, 16)}, device_id_type=MESH)
        pl.semaphore_signal(barrier, inc=1, device_id={"dp": lax.rem(dpi + d, 16)}, device_id_type=MESH)

    pair = pl.ds(pl.multiple_of(lax.div(sp, 2) * 128, 128), 128)
    lo, hi = join(wq_ref[:, pair], wk_ref[:, pair])
    wpk[...] = jnp.where(lax.rem(sp, 2) == 0, lo, hi)

    for p in range(8):
        lanes = slice(p * 128, (p + 1) * 128)
        vgpack[2 * p], vgpack[2 * p + 1] = join(v_ref[:, lanes], g_ref[:, lanes])

    pl.semaphore_wait(barrier, 30)

    sends = []

    def send(src, dst, ss, rs, to, when=None):
        def make():
            return pltpu.make_async_remote_copy(src_ref=src(), dst_ref=dst(), send_sem=ss(), recv_sem=rs(), device_id=to(),
                                                device_id_type=MESH)
        make().start()
        sends.append((make, when))

    def arrive(dst, ss, rs):
        pltpu.make_async_remote_copy(src_ref=dst, dst_ref=dst, send_sem=ss, recv_sem=rs, device_id={"sp": sp},
                                     device_id_type=MESH).wait_recv()

    def rows_of(i, n, at=0, size=None):
        return pl.ds(pl.multiple_of(i * n + at, 16), size or n)

    def t1_go(d):
        return {"sp": spot(u, w + 1 - 2 * d)}

    def t1_part(d, i):
        back = 1 if i < 2 else 2
        half = d if i != 1 else 1 - d
        return rows_of(spot(u, w - back if d == 0 else w + back), TOK, half * HALF, HALF)

    def t1_send(d, i):
        if i < 2:
            half = d if i == 0 else 1 - d
            send(lambda: tok_ref.at[pl.ds(half * HALF, HALF)], lambda: tokF.at[rows_of(sp, TOK, half * HALF, HALF)],
                 lambda: t1s.at[d, i], lambda: t1r.at[d, i], lambda: t1_go(d))
        else:
            send(lambda: tokF.at[t1_part(d, 0)], lambda: tokF.at[t1_part(d, 0)], lambda: t1s.at[d, i], lambda: t1r.at[d, i], lambda: t1_go(d))

    def t1_wait(d, i):
        arrive(tokF.at[t1_part(d, i)], t1s.at[d, i], t1r.at[d, i])

    def t2_go(d):
        return {"sp": spot(u + 1 - 2 * d, w)}

    def t2_rows(d, back, i, half):
        return rows_of(spot(u - back if d == 0 else u + back, w + i), TOK, half * HALF, HALF)

    def t2_send(d, i, k):
        half = d if k != 1 else 1 - d
        part = lambda: tokF.at[t2_rows(d, 1 if k == 2 else 0, i, half)]
        src = (lambda: tok_ref.at[pl.ds(half * HALF, HALF)]) if i == 0 and k < 2 else part
        send(src, part, lambda: t2s.at[d, i, k], lambda: t2r.at[d, i, k], lambda: t2_go(d))

    def t2_wait(d, i, k):
        arrive(tokF.at[t2_rows(d, 2 if k == 2 else 1, i, d if k != 1 else 1 - d)], t2s.at[d, i, k], t2r.at[d, i, k])

    def t2_event(i):
        for d in range(2):
            t2_wait(d, i, 0)
            t2_send(d, i, 2)

    def t2_end():
        for i in range(4):
            for d in range(2):
                t2_wait(d, i, 1)
                t2_wait(d, i, 2)

    def lane_block(i):
        return pl.ds(pl.multiple_of(i * 128, 128), 128)

    def p1_send():
        for d in range(1, 8):
            send(lambda: wpk, lambda: wh4.at[rows_of(dpi, 128), lane_block(u)], lambda d=d: p1s.at[d], lambda d=d: p1r.at[d],
                 lambda d=d: {"dp": lax.rem(z + d, 8) * 2 + core})
        send(lambda: wpk, lambda: wh4.at[rows_of(dpi, 128), lane_block(w)], lambda: m1s.at[0], lambda: m1r.at[0], lambda: {"dp": mate})

    def p1_wait():
        for d in (1, 7, 2, 6, 3, 5, 4):
            part = lambda d=d: wh4.at[rows_of(lax.rem(z + 8 - d, 8) * 2 + core, 128), lane_block(u)]
            to = lambda d=d: wh4.at[rows_of(lax.rem(z + 8 - d, 8) * 2 + core, 128), lane_block(w)]
            arrive(part(), p1s.at[d], p1r.at[d])
            send(part, to, lambda d=d: m1s.at[d], lambda d=d: m1r.at[d], lambda: {"dp": mate})
        for d in range(8):
            arrive(wh4.at[rows_of(lax.rem(z + 8 - d, 8) * 2 + 1 - core, 128), lane_block(u)], m1s.at[d], m1r.at[d])

    def h_part(back, d, half):
        return wh4.at[pl.ds(half * 1024, 1024), lane_block(lax.rem(u + 4 - back if d == 0 else u + back, 4))]

    def h_send(d, i):
        half = d if i != 1 else 1 - d
        part = lambda: h_part(0 if i < 2 else 1, d, half)
        send(part, part, lambda: hs.at[d, i], lambda: hr.at[d, i], lambda: t2_go(d))

    def h_wait(d, i):
        arrive(h_part(1 if i < 2 else 2, d, d if i != 1 else 1 - d), hs.at[d, i], hr.at[d, i])

    wF = (wqF, wkF)
    wown = (wq_ref, wk_ref)

    def w_go(d):
        return {"dp": lax.rem(z + 1 + 6 * d, 8) * 2 + core}

    def w_owner(back, d):
        return lax.rem(z + 8 - back if d == 0 else z + back, 8) * 2 + core

    def w_which(d, k):
        return d if k == 6 else k % 2

    def w_send(d, k):
        m = w_which(d, k)
        send(lambda: wown[m] if k < 2 else wF[m].at[rows_of(w_owner(k // 2, d), 128)], lambda: wF[m].at[rows_of(w_owner(k // 2, d), 128)],
             lambda: wsend.at[d, k], lambda: wrecv.at[d, k], lambda: w_go(d))

    def mate_own(m):
        send(lambda: wown[m], lambda: wF[m].at[rows_of(dpi, 128)], lambda: psend.at[14 + m], lambda: precv.at[14 + m], lambda: {"dp": mate})

    def w_event(k):
        for d in range(2):
            m = w_which(d, k)
            part = lambda m=m, d=d: wF[m].at[rows_of(w_owner(k // 2 + 1, d), 128)]
            arrive(part(), wsend.at[d, k], wrecv.at[d, k])
            if k < 4 or k == 4 + d:
                w_send(d, k + 2 if k < 4 else 6)
            send(part, part, lambda d=d: psend.at[d * 7 + k], lambda d=d: precv.at[d * 7 + k], lambda: {"dp": mate})

    def mate_end():
        for m in range(2):
            arrive(wF[m].at[rows_of(mate, 128)], psend.at[14 + m], precv.at[14 + m])
        for k in range(7):
            for d in range(2):
                arrive(wF[w_which(d, k)].at[rows_of(w_owner(k // 2 + 1, d) + 1 - 2 * core, 128)], psend.at[d * 7 + k], precv.at[d * 7 + k])

    def vg_send():
        for d in range(1, 16):
            send(lambda d=d: vgpack.at[lax.rem(sp + d, 16)], lambda: vgF.at[rows_of(sp, TOK)], lambda d=d: asend.at[d], lambda d=d: arecv.at[d],
                 lambda d=d: {"sp": lax.rem(sp + d, 16)})

    def vg_wait():
        for d in range(1, 16):
            arrive(vgF.at[rows_of(lax.rem(sp + 16 - d, 16), TOK)], asend.at[d], arecv.at[d])

    def qk_send(i):
        for du in (1, 3, 2):
            send(lambda du=du: qkS.at[lax.rem(u + du, 4), i], lambda: rot.at[rows_of(spot(u, w + i), TOK)],
                 lambda du=du: qs.at[du, i], lambda du=du: qr.at[du, i], lambda du=du: {"sp": spot(u + du, w)})

    def qk_wait():
        for du in range(1, 4):
            for i in range(4):
                arrive(rot.at[rows_of(spot(u - du, w + i), TOK)], qs.at[du, i], qr.at[du, i])

    for i in range(2):
        for d in range(2):
            t1_send(d, i)
    p1_send()
    for d in range(2):
        t2_send(d, 0, 0)
    own = [pltpu.make_async_copy(tok_ref, tokF.at[rows_of(sp, TOK)], lsem.at[0]),
           pltpu.make_async_copy(wq_ref, wqF.at[rows_of(dpi, 128)], lsem.at[1]),
           pltpu.make_async_copy(wk_ref, wkF.at[rows_of(dpi, 128)], lsem.at[2])]
    for c in own:
        c.start()
    wh4[rows_of(dpi, 128), lane_block(u)] = wpk[...]
    vgF[rows_of(sp, TOK), :] = vgpack[sp]

    def tables(i, _):
        cols = pl.ds(pl.multiple_of(i * 128, 128), 128)
        c, s = cosT[:, cols], sinT[:, cols]
        tabC[cols, :] = jnp.concatenate([c] * 8, axis=0).T
        tabS[cols, :] = jnp.concatenate([-s, s] * 4, axis=0).T
        return 0
    lax.fori_loop(0, SEQ // 128, tables, 0)
    for c in own:
        c.wait()

    for d in range(2):
        t1_wait(d, 0)
        t1_send(d, 2)
    p1_wait()
    for i in range(2):
        for d in range(2):
            h_send(d, i)
    for d in range(2):
        t1_wait(d, 1)
        t1_wait(d, 2)
    for d in range(2):
        h_wait(d, 0)
        h_send(d, 2)
    vg_send()
    for d in range(2):
        t2_send(d, 0, 1)
    for k in range(2):
        for d in range(2):
            w_send(d, k)
    for m in range(2):
        mate_own(m)
    for d in range(2):
        h_wait(d, 1)
        h_wait(d, 2)

    lane16 = lax.rem(lax.broadcasted_iota(jnp.int32, (TOK, 128), 1), 32) < 16

    def project(i):
        rows = [rows_of(spot(u, w + i + n), TOK) for n in range(2)]
        r = mm(jnp.concatenate([tokF[p, :] for p in rows], axis=0), wh4[...])
        for n in range(2):
            c, s = tabC[rows[n], :], tabS[rows[n], :]
            for h in range(4):
                a = r[n * TOK:(n + 1) * TOK, h * 128:(h + 1) * 128]
                other = jnp.where(lane16, pltpu.roll(a, 112, 1), pltpu.roll(a, 16, 1))
                qkS[h, i + n] = (a * c + other * s).astype(BF16)

    project(0)
    qk_send(0)
    project(2)
    for i in range(1, 4):
        qk_send(i)
    for i in range(4):
        rot[rows_of(spot(u, w + i), TOK), :] = qkS[u, i]
    for i in range(1, 4):
        for k in range(2):
            for d in range(2):
                t2_send(d, i, k)
    w_event(0)
    vg_wait()

    def turn_vg(i, _):
        r = pl.multiple_of(i * 256, 256)
        vgT[:, pl.ds(r, 256)] = vgF[pl.ds(r, 256), :].astype(F32).T.astype(BF16)
        return 0
    lax.fori_loop(0, SEQ // 256, turn_vg, 0)
    qk_wait()

    def turn_qk(i, _):
        r = pl.multiple_of(i * 256, 256)
        rotT[:, pl.ds(r, 256)] = rot[pl.ds(r, 256), :].astype(F32).T.astype(BF16)
        return 0
    lax.fori_loop(0, SEQ // 256, turn_qk, 0)

    def back_send():
        for d in (10, 2, 8, 5, 7, 9, 11, 6, 14, 3, 13, 1, 4, 12, 15):
            send(lambda d=d: bpack.at[lax.rem(sp + d, 16)], lambda: bF.at[sp], lambda d=d: bsend.at[d], lambda d=d: brecv.at[d],
                 lambda d=d: {"sp": lax.rem(sp + d, 16)})

    plan = {
        (0, 0): [lambda: w_event(1)],
        (0, 1): [lambda: w_event(2), lambda: t2_event(0)],
        (1, 0): [lambda: w_event(3), lambda: t2_event(1)],
        (1, 1): [lambda: w_event(4), lambda: t2_event(2)],
        (2, 0): [lambda: w_event(5), lambda: t2_event(3)],
        (3, 0): [lambda: w_event(6)],
    }

    def hook(step, place):
        for (s, p), jobs in plan.items():
            if p == place:
                @pl.when(step == s)
                def _():
                    for job in jobs:
                        job()

    def done(step, b):
        for i in range(BQ // 256):
            cols = pl.ds(pl.multiple_of(b * BQ + i * 256, 256), 256)
            c, s = cosT[:, cols], sinT[:, cols]
            bt = jnp.concatenate([rot_t(dqT[:, cols], c, s, -1.0), rot_t(acc[0:64, cols], c, s, -1.0)], axis=0)
            backT[:, cols] = bt.astype(BF16)
            xf[cols, :] = bt.T
            xv[cols, :] = acc[64:128, cols].T

        first = jnp.where(step == NB - 1, 0, 13 - 3 * step)

        def pack(k, _):
            i = first + k
            r = pl.multiple_of(i * TOK, TOK)
            bpack[i, 0:TOK, :] = xf[pl.ds(r, TOK), :].astype(BF16)
            bpack[i, TOK:TOK + HALF, :] = jnp.concatenate([xv[pl.ds(r, HALF), :], xv[pl.ds(r + HALF, HALF), :]], axis=1).astype(BF16)
            return 0
        lax.fori_loop(0, jnp.where(step == NB - 1, 4, 3), pack, 0)

    attention(lam_ref[sp], rot, rotT, vgF, vgT, cosT, sinT, dqT, acc, e1, e2, mix, dp, hook, done)
    t2_end()
    back_send()

    far = (4, 3, 5, 2, 6, 1, 7, 0)

    def chip(i):
        return lax.rem(z + far[i], 8)

    def piece(i):
        r = mm(backT[...], tokF[:, pl.ds(pl.multiple_of(chip(i) * 256, 256), 256)]).astype(BF16)
        dwp[0, chip(i)] = r[:, :128]
        dwp[1, chip(i)] = r[:, 128:]

    def piece_mate(i):
        send(lambda: dwp.at[1 - core, chip(i)], lambda: dwM.at[chip(i)], lambda: rsend.at[8 + i], lambda: rrecv.at[8 + i], lambda: {"dp": mate})

    def piece_add(i):
        arrive(dwM.at[chip(i)], rsend.at[8 + i], rrecv.at[8 + i])
        both = (dwp[core, chip(i)].astype(F32) + dwM[chip(i)].astype(F32)).astype(BF16)
        dwP[chip(i)] = both
        if far[i] == 0:
            dwR[z] = both

    def piece_go(i):
        if far[i]:
            send(lambda: dwP.at[chip(i)], lambda: dwR.at[z], lambda: rsend.at[far[i]], lambda: rrecv.at[far[i]], lambda: {"dp": chip(i) * 2 + core})

    for t in range(15):
        for job, late in ((piece, 0), (piece_mate, 1), (piece_add, 5), (piece_go, 6)):
            if 0 <= t - late < 8:
                job(t - late)
    bF[sp] = bpack[sp]
    mate_end()
    for d in range(1, 8):
        arrive(dwR.at[lax.rem(z + 8 - d, 8)], rsend.at[d], rrecv.at[d])
    total = dwR[0].astype(F32)
    for i in range(1, 8):
        total += dwR[i].astype(F32)
    total = total.T.astype(BF16)
    dwS[...] = total
    dwG[sp] = total

    def row_send(dw):
        send(lambda: dwS, lambda: dwG.at[sp], lambda: gsend.at[dw], lambda: grecv.at[dw], lambda: {"sp": spot(u, w + dw)})

    def column_send(i):
        for du in (2, 1, 3):
            send(lambda: dwS if i == 0 else dwG.at[spot(u, w - i)], lambda: dwG.at[spot(u, w - i)], lambda du=du: g2send.at[du, i],
                 lambda du=du: g2recv.at[du, i], lambda du=du: {"sp": spot(u + du, w)})

    for dw in (2, 1, 3):
        row_send(dw)
    column_send(0)
    for d in range(1, 16):
        arrive(bF.at[lax.rem(sp + 16 - d, 16)], bsend.at[d], brecv.at[d])

    bq, bk = [], []
    for p in range(8):
        lanes = slice(p * 128, (p + 1) * 128)
        a, b = bF[2 * p], bF[2 * p + 1]
        q, k = join(a[:TOK], b[:TOK])
        bq.append(q)
        bk.append(k)
        top, low = join(a[TOK:], b[TOK:])
        vgrad_ref[0:HALF, lanes] = top
        vgrad_ref[HALF:TOK, lanes] = low
    bq = jnp.concatenate(bq, axis=1)
    bk = jnp.concatenate(bk, axis=1)
    for i in (1, 3, 2):
        arrive(dwG.at[spot(u, w - i)], gsend.at[i], grecv.at[i])
        column_send(i)
    for n in range(8):
        rows = slice(n * 256, (n + 1) * 256)
        tg_ref[:, rows] = (mm(bq, wqF[rows, :], TRANS_B) + mm(bk, wkF[rows, :], TRANS_B)).astype(BF16)

    for i in range(4):
        for du in range(1, 4):
            arrive(dwG.at[spot(u - du, w - i)], g2send.at[du, i], g2recv.at[du, i])
    dw_ref[...] = dwG[...]
    for make, when in sends:
        if when is None:
            make().wait_send()
        else:
            pl.when(when())(lambda make=make: make().wait_send())


def settle(factor, tg_hbm, vg_hbm, dw_hbm, tg_out, vg_out, dwq_out, dwk_out, tg_ref, vg_ref, dw_ref, sem):
    dw_in = pltpu.make_async_copy(dw_hbm, dw_ref, sem.at[0])
    tg_in = pltpu.make_async_copy(tg_hbm, tg_ref, sem.at[1])
    vg_in = pltpu.make_async_copy(vg_hbm, vg_ref, sem.at[2])
    tg_go = pltpu.make_async_copy(tg_ref, tg_out, sem.at[3])
    vg_go = pltpu.make_async_copy(vg_ref, vg_out, sem.at[4])
    for c in (dw_in, tg_in, vg_in):
        c.start()
    tg_in.wait()
    tg_go.start()
    vg_in.wait()
    vg_go.start()
    dw_in.wait()
    for p in range(8):
        lanes = slice(p * 128, (p + 1) * 128)
        q, k = join(dw_ref[2 * p].astype(F32), dw_ref[2 * p + 1].astype(F32))
        dwq_out[:, lanes] = q * factor
        dwk_out[:, lanes] = k * factor
    tg_go.wait()
    vg_go.wait()


def body(tokens, query_weight, key_weight, values, lambdas, out_grad):
    half = DQK // 2
    freqs = np.exp(np.float32(-math.log(THETA)) * np.arange(half, dtype=np.float32) / np.float32(half))
    angles = freqs[:, None] * np.arange(SEQ, dtype=np.float32)[None, :]
    vm = pl.BlockSpec(memory_space=pltpu.VMEM)
    dma = pltpu.SemaphoreType.DMA
    V = pltpu.VMEM
    return_shapes = (
        jax.ShapeDtypeStruct((TOK, D), BF16),
        jax.ShapeDtypeStruct((TOK, COLS), BF16),
        jax.ShapeDtypeStruct((16, 128, 128), BF16),
    )
    raw = pl.pallas_call(
        kernel,
        out_shape=return_shapes,
        in_specs=[pl.BlockSpec(memory_space=pltpu.SMEM)] + [vm] * 7,
        out_specs=(vm,) * 3,
        scratch_shapes=[
            V((SEQ, D), BF16), V((D, COLS), BF16), V((D, COLS), BF16), V((D, 512), BF16), V((128, 128), BF16),
            V((SEQ, 128), F32), V((SEQ, 128), F32), V((4, 4, TOK, 128), BF16), V((SEQ, 128), F32), V((SEQ, 64), F32),
            V((16, TOK, 128), BF16), V((SEQ, 128), BF16),
            V((SEQ, 128), BF16), V((128, SEQ), BF16), V((128, SEQ), BF16), V((64, SEQ), F32), V((128, SEQ), F32),
            V((SEQ, BQ), F32), V((SEQ, BQ), F32), V((SEQ, BQ), BF16), V((SEQ, BQ), F32),
            V((128, SEQ), BF16), V((16, TOK + HALF, 128), BF16), V((16, TOK + HALF, 128), BF16),
            V((2, 8, 128, 128), BF16), V((8, 128, 128), BF16), V((8, 128, 128), BF16), V((8, 128, 128), BF16), V((128, 128), BF16), V((16, 128, 128), BF16),
            dma((2, 3)), dma((2, 3)), dma((2, 4, 3)), dma((2, 4, 3)), dma((8,)), dma((8,)), dma((8,)), dma((8,)),
            dma((2, 3)), dma((2, 3)), dma((4, 4)), dma((4, 4)),
            dma((2, 7)), dma((2, 7)), dma((16,)), dma((16,)), dma((16,)), dma((16,)),
            dma((16,)), dma((16,)), dma((16,)), dma((16,)), dma((4,)), dma((4,)), dma((4, 4)), dma((4, 4)), dma((3,)),
        ],
        compiler_params=pltpu.CompilerParams(vmem_limit_bytes=62 * 1024 * 1024, collective_id=0, has_side_effects=True),
        name="differential_backward",
    )(lambdas, tokens[0], query_weight, key_weight, values[0], out_grad[0], jnp.asarray(np.cos(angles)), jnp.asarray(np.sin(angles)))
    tg, vg, dq, dk = pl.pallas_call(
        functools.partial(settle, 1.0 / math.sqrt(16 * SEQ)),
        out_shape=(jax.ShapeDtypeStruct((TOK, D), BF16), jax.ShapeDtypeStruct((TOK, COLS), BF16),
                   jax.ShapeDtypeStruct((128, COLS), F32), jax.ShapeDtypeStruct((128, COLS), F32)),
        in_specs=[pl.BlockSpec(memory_space=pl.ANY)] * 3,
        out_specs=(pl.BlockSpec(memory_space=pl.ANY),) * 2 + (vm,) * 2,
        scratch_shapes=[V((TOK, D), BF16), V((TOK, COLS), BF16), V((16, 128, 128), BF16), dma((5,))],
        name="settle",
    )(*raw)
    return tg[None], vg[None], dq, dk


def solution(mesh):
    in_specs = (
        P("dp", "sp", None),
        P("dp", None),
        P("dp", None),
        P("dp", "sp", None),
        P(),
        P("dp", "sp", None),
    )
    out_specs = (P("dp", "sp", None), P("dp", "sp", None), P("dp", None), P("dp", None))
    return jax.shard_map(body, mesh=mesh, in_specs=in_specs, out_specs=out_specs, check_vma=False)
```
